32 devices in a mesh: ep: 8 (over z, x), tp: 4 (over y, core).
Axes of the slice: x: 2, y: 2, z: 4, core: 2. Of those that a mesh axis runs over, the one named last changes fastest.
Arguments:
- tokens: bfloat16 [4096, 4096], P('ep', 'tp'), may hold values from -60 to 60
- routes: int32 [4096, 4], P('ep'), may hold values from 0 to 31, all different within a row; in each aligned block of 512 rows (0 to 511, 512 to 1023, ...) at most 128 rows name the same one
- route_weights: float32 [4096, 4], P('ep'), may hold values from 0.1 to 1
- pre_gain: float32 [4096], P('tp'), may hold values from 0.1 to 1.9
- expert_gate: bfloat16 [32, 4096, 512], P('ep', 'tp'), may hold values from -0.09375 to 0.09375
- expert_up: bfloat16 [32, 4096, 512], P('ep', 'tp'), may hold values from -0.09375 to 0.09375
- expert_down: bfloat16 [32, 512, 4096], P('ep', None, 'tp'), may hold values from -1 to 1
- shared_gate: bfloat16 [4096, 512], P('tp'), may hold values from -0.09375 to 0.09375
- shared_up: bfloat16 [4096, 512], P('tp'), may hold values from -0.09375 to 0.09375
- shared_down: bfloat16 [512, 4096], P(None, 'tp'), may hold values from -1 to 1
- post_gain: float32 [4096], P('tp'), may hold values from 0.1 to 1.9
Outputs:
- layer_out: bfloat16 [4096, 4096], P('ep', 'tp')
The draws below stay inside these ranges and needn't reach their ends.
Inputs may be any that keep to these rules, and one draw needn't show every extreme that they name: `routes`: each row names 4 different experts. Within each aligned block of 512 rows (the tokens of one index of ep) no expert is named more than 128 times, a bound that some block reaches.
All inputs are finite; a program needn't handle non-finite values.
Results may differ from the reference program's by a relative error of at most 0.022.
Values may be sent and summed in bfloat16 or wider, within the bound.
A program may use at most 128 MiB of HBM per device.

```python
import math
import jax
import jax.numpy as jnp
import numpy as np
from jax import lax

D = 4096
FF = 512
FS = 512
TOPK = 4
TOK_EP = 512
EXPERTS = 32
TOKENS = 4096
CAP = 128
N_EP = 8
N_TP = 4


def draw_tokens(key, part):
    key_base, key_rows, key_cols = jax.random.split(key, 3)
    ramp = 3.0 ** (jnp.arange(D, dtype=jnp.float32) / D)
    columns = ramp * jax.random.uniform(key_cols, (D,), jnp.float32, 0.5, 2.0)
    scales = jnp.exp(jax.random.uniform(key_rows, (TOKENS, 1), jnp.float32, -1.0, 1.0))
    base = jnp.clip(jax.random.normal(key_base, (TOKENS, D), jnp.float32), -6.0, 6.0)
    return jnp.clip(base * scales * columns, -60.0, 60.0).astype(jnp.bfloat16)


def ramped_weight(key, shape, fan_in):
    key_base, key_cols = jax.random.split(key)
    ramp = 3.0 ** (jnp.arange(D, dtype=jnp.float32) / D)
    columns = ramp * jax.random.uniform(key_cols, (D,), jnp.float32, 0.5, 2.0) / 2.0
    base = jnp.clip(jax.random.normal(key_base, shape, jnp.float32), -6.0, 6.0) * fan_in ** (-0.5)
    return jnp.clip(base * columns, -1.0, 1.0).astype(jnp.bfloat16)


def draw_expert_down(key, part):
    return ramped_weight(key, (EXPERTS, FF, D), FF)


def draw_shared_down(key, part):
    return ramped_weight(key, (FS, D), FS)


def steps_of(rng, dims, cuts, low, top_value):
    def one(position, shards_of):
        steps = jax.random.uniform(jax.random.fold_in(jax.random.fold_in(rng, 6), position), (shards_of,), jnp.float32, low / len(cuts), top_value / len(cuts))
        return jnp.repeat(jnp.exp(steps), dims[position] // shards_of).reshape((-1,) + (1,) * (len(dims) - position - 1))

    factor_of = one(*cuts[0])
    for cut in cuts[1:]:
        factor_of = factor_of * one(*cut)
    return factor_of


def routed_block(rng, own, number, rows, number_of, top, limit, slope):
    ranking = jax.random.permutation(rng, number_of)
    heavy_load, usual = shares(number_of, rows * top, limit, slope, True), shares(number_of, rows * top, limit, slope, False)
    places = jnp.arange(number_of)

    def named(sizes, offset_by):
        used = int((sizes > 0).sum())
        fixed = max(1, used // 4)
        moved = fixed + (places - fixed + offset_by * (used - fixed)) % max(1, number_of - fixed)
        return jnp.zeros((number_of,), jnp.int32).at[ranking[jnp.where(places < fixed, places, moved)]].set(jnp.asarray(sizes, jnp.int32))

    sizes = jnp.where(number % 4 == 0, named(heavy_load, number // 4), named(usual, number - number // 4 - 1))
    mixed = jax.random.permutation(jax.random.fold_in(own, 3), number_of)
    source_of, sink = mixed[0:number_of // 2 * 2:2], mixed[1:number_of // 2 * 2:2]
    slack = jnp.minimum(sizes[source_of] - 1, limit - sizes[sink]) // 2
    slack = jnp.where((source_of == ranking[0]) | (sink == ranking[0]) | (sizes[sink] == 0), 0, jnp.maximum(slack, 0))
    moved = jax.random.randint(jax.random.fold_in(own, 4), (number_of // 2,), 0, 1 << 20) % (slack + 1)
    sizes = sizes.at[source_of].add(-moved).at[sink].add(moved)
    labels = jnp.searchsorted(jnp.cumsum(sizes), jnp.arange(rows * top), side="right").astype(jnp.int32)
    table = labels.reshape(top, rows).T
    table = table[jax.random.permutation(jax.random.fold_in(own, 1), rows)]
    offset_by = jax.random.randint(jax.random.fold_in(own, 2), (rows, 1), 0, top)
    return jnp.take_along_axis(table, (jnp.arange(top)[None, :] + offset_by) % top, axis=1)


def shares(count, total, reach, lean, full):
    portions = [(1 << 20) // math.isqrt(grade ** lean) + 1 for grade in range(1, count + 1)]
    largest = reach if full else min(reach, max(-(-total // count), total * portions[0] // sum(portions)))
    least = 1 if total - largest >= count - 1 else 0
    counts, surplus = [largest] + [least] * (count - 1), total - largest - least * (count - 1)
    while surplus > 0:
        candidates = [i for i in range(1, count) if counts[i] < largest] or [i for i in range(1, count) if counts[i] < reach]
        mass, budget = sum([portions[i] for i in candidates]), surplus
        for i in candidates:
            extra = min(reach - counts[i], max(1, budget * portions[i] // mass), surplus)
            counts[i] = counts[i] + extra
            surplus = surplus - extra
    return np.array(counts)


def centred(rng, shape, width, reach, cuts=(), kind=jnp.bfloat16):
    gain = steps_of(rng, shape, cuts, -0.22, 0.18) if cuts else 1.0
    drawn = jax.random.normal(rng, shape, jnp.float32) * width * gain
    return jnp.minimum(jnp.maximum(drawn, -reach), reach).astype(kind)


def setup_inputs(seed: int = 0) -> dict:
    streams_of = jax.random.split(jax.random.key(seed), 12)
    tokens = draw_tokens(jax.random.fold_in(streams_of[11], 71), 0)
    routes_keys = jax.random.split(jax.random.fold_in(streams_of[1], 1), TOKENS // TOK_EP)
    routes_turns = jax.random.permutation(jax.random.fold_in(streams_of[1], 3), TOKENS // TOK_EP)
    routes = jax.vmap(lambda own, number: routed_block(jax.random.fold_in(streams_of[1], 2), own, number, TOK_EP, EXPERTS, TOPK, CAP, 2))(routes_keys, routes_turns).reshape((TOKENS, TOPK))
    route_weights = jnp.clip(jnp.exp(math.log(1.0) - 2.3025851 * jax.random.uniform(streams_of[2], (TOKENS, TOPK), jnp.float32) ** steps_of(streams_of[2], (TOKENS, TOPK), ((0, 8),), -0.2, 0.2)), 0.1, 1.0)
    pre_gain = jnp.clip(1.0 + 0.18 * jax.random.normal(streams_of[3], (D,), jnp.float32), 0.1, 1.9)
    expert_gate = centred(streams_of[4], (EXPERTS, D, FF), D ** -0.5, 0.09375, ((0, 8), (1, 4)))
    expert_up = centred(streams_of[5], (EXPERTS, D, FF), D ** -0.5, 0.09375, ((0, 8), (1, 4)))
    expert_down = draw_expert_down(jax.random.fold_in(streams_of[11], 71), 0)
    shared_gate = centred(streams_of[7], (D, FS), D ** -0.5, 0.09375, ((0, 4),))
    shared_up = centred(streams_of[8], (D, FS), D ** -0.5, 0.09375, ((0, 4),))
    shared_down = draw_shared_down(jax.random.fold_in(streams_of[11], 71), 0)
    post_gain = jnp.clip(1.0 + 0.18 * jax.random.normal(streams_of[10], (D,), jnp.float32), 0.1, 1.9)
    return {"tokens": tokens, "routes": routes, "route_weights": route_weights, "pre_gain": pre_gain, "expert_gate": expert_gate, "expert_up": expert_up, "expert_down": expert_down, "shared_gate": shared_gate, "shared_up": shared_up, "shared_down": shared_down, "post_gain": post_gain}


epsilon = 1e-06

def inverse_norm(values):
    return lax.rsqrt(lax.optimization_barrier(jnp.mean(values * values, axis=1)) + epsilon)

def blocked_product(inputs, weight):
    row_count = inputs.shape[0]
    out_width = weight.shape[1]
    pieces = inputs.reshape(row_count, N_TP, D // N_TP).astype(jnp.float32)
    blocks = weight.reshape(N_TP, D // N_TP, out_width).astype(jnp.float32)
    partial_value = jnp.einsum('rnd,ndf->nrf', pieces, blocks)
    rounded = lax.optimization_barrier(partial_value.astype(jnp.bfloat16))
    return lax.optimization_barrier(jnp.sum(rounded.astype(jnp.float32), axis=0))

def reference(tokens, routes, route_weights, pre_gain, expert_gate, expert_up, expert_down, shared_gate, shared_up, shared_down, post_gain):
    inputs = tokens.astype(jnp.float32)
    normed = (inputs * inverse_norm(inputs)[:, None] * pre_gain.astype(jnp.float32)).astype(jnp.bfloat16)
    per_block = TOK_EP * TOPK
    flat_ids = routes.reshape(N_EP, per_block).astype(jnp.int32)
    one_hot = (flat_ids[:, :, None] == jnp.arange(EXPERTS, dtype=jnp.int32)[None, None, :]).astype(jnp.int32)
    slots = lax.optimization_barrier(jnp.sum(jnp.cumsum(one_hot, axis=1) * one_hot, axis=2)) - 1
    sources = jnp.arange(N_EP, dtype=jnp.int32)[:, None]
    positions = (sources * CAP + slots).reshape(-1).astype(jnp.int32)
    token_index = (sources * TOK_EP + jnp.arange(per_block, dtype=jnp.int32)[None, :] // TOPK).reshape(-1).astype(jnp.int32)
    expert_index = flat_ids.reshape(-1)
    token_table = jnp.full((EXPERTS, N_EP * CAP), TOKENS, jnp.int32).at[expert_index, positions].set(token_index)
    weight_table = jnp.zeros((EXPERTS, N_EP * CAP), jnp.float32).at[expert_index, positions].set(route_weights.reshape(-1).astype(jnp.float32))

    def expert_step(totals, stacked):
        table_rows, table_weights, gate_weight, up_weight, down_weight = stacked
        arrived = jnp.take(normed, table_rows, axis=0, mode='fill', fill_value=0)
        gate_pre = blocked_product(arrived, gate_weight)
        up_pre = blocked_product(arrived, up_weight)
        hidden = (jax.nn.silu(gate_pre) * up_pre).astype(jnp.bfloat16)
        expert_out = jnp.dot(hidden, down_weight, preferred_element_type=jnp.float32).astype(jnp.bfloat16)
        totals = totals.at[table_rows].add(table_weights[:, None] * expert_out.astype(jnp.float32), mode='drop')
        return (totals, None)
    routed, _ = lax.scan(expert_step, jnp.zeros((TOKENS, D), jnp.float32), (token_table, weight_table, expert_gate, expert_up, expert_down))
    shared_gate_pre = blocked_product(normed, shared_gate)
    shared_up_pre = blocked_product(normed, shared_up)
    shared_hidden = (jax.nn.silu(shared_gate_pre) * shared_up_pre).astype(jnp.bfloat16)
    shared_out = jnp.dot(shared_hidden, shared_down, preferred_element_type=jnp.float32).astype(jnp.bfloat16)
    mixture = routed + shared_out.astype(jnp.float32)
    return (mixture * inverse_norm(mixture)[:, None] * post_gain.astype(jnp.float32)).astype(jnp.bfloat16)
```

```python
import functools

import jax
import jax.numpy as jnp
from jax import lax
from jax.experimental import pallas as pl
from jax.experimental.pallas import tpu as pltpu
from jax.sharding import PartitionSpec as P

epsilon = 1e-06
MESH = pl.DeviceIdType.MESH
F32, BF16 = jnp.float32, jnp.bfloat16
CHUNKS = 4
TABLE = 16
COLUMNS = 256


def ring_of(groups, width):
    if width < 2 or groups % width or groups // width < 2:
        return list(range(groups))
    depth = groups // width
    cycle = []
    for x in range(width):
        column = range(1, depth) if x % 2 == 0 else range(depth - 1, 0, -1)
        cycle += [z * width + x for z in column]
    return cycle + [x for x in range(width - 1, -1, -1)]


def dot(a, b):
    return jnp.dot(a, b, preferred_element_type=F32)


def dot_nt(a, b):
    return lax.dot_general(a, b, (((1,), (1,)), ((), ())), preferred_element_type=F32)


def iota(shape, axis):
    return lax.broadcasted_iota(jnp.int32, shape, axis).astype(F32)


def layer_kernel(
    cfg,
    tokens_hbm,
    meta_ref,
    gain_ref,
    gate_hbm,
    up_hbm,
    down_hbm,
    sgate_hbm,
    sup_hbm,
    sdown_hbm,
    post_ref,
    out_ref,
    tok,
    xbuf,
    mbuf,
    gate,
    up,
    down,
    sgate,
    sup,
    sdown,
    rows,
    hits,
    parts,
    got1,
    sums,
    got2,
    hid,
    made,
    back,
    farb,
    mix,
    slotv,
    wv,
    rinv,
    rwt,
    earlier,
    eye,
    squares,
    load_sem,
    gs,
    gr,
    ms,
    mr,
    rs,
    rr,
    s1s,
    s1r,
    s2s,
    s2r,
    s3s,
    s3r,
    s4s,
    s4r,
    ns,
    nr,
    credit,
):
    groups, members, experts, cap, fanout, ring, features = cfg
    count, width = out_ref.shape
    reach = groups // 2
    wide = members // 2
    units = gate.shape[2]
    share = units // members
    chunk = count // CHUNKS
    slots = experts * cap
    far = 2 * reach - 1

    group, me = lax.axis_index("ep"), lax.axis_index("tp")
    core, row = lax.rem(me, 2), lax.div(me, 2)
    ahead, behind = jnp.int32(0), jnp.int32(0)
    for i, place in enumerate(ring):
        here = group == place
        ahead = jnp.where(here, ring[(i + 1) % groups], ahead)
        behind = jnp.where(here, ring[(i - 1) % groups], behind)
    gather_to = ({"ep": ahead}, {"ep": behind})
    return_to = ({"ep": behind}, {"ep": ahead})
    partner = {"tp": row * 2 + 1 - core}

    def peer_row(d):
        return lax.rem(row + d, wide)

    def remote(src, dst, send, recv, to):
        return pltpu.make_async_remote_copy(
            src_ref=src, dst_ref=dst, send_sem=send, recv_sem=recv, device_id=to, device_id_type=MESH
        )

    barrier = pltpu.get_barrier_semaphore()
    for to in gather_to:
        pl.semaphore_signal(barrier, inc=1, device_id=to, device_id_type=MESH)
    for d in range(1, members):
        pl.semaphore_signal(
            barrier, inc=1, device_id={"tp": lax.rem(me + d, members)}, device_id_type=MESH
        )

    loads = [
        pltpu.make_async_copy(src, dst, load_sem.at[i])
        for i, (src, dst) in enumerate(
            (
                (tokens_hbm, tok),
                (gate_hbm, gate),
                (up_hbm, up),
                (sgate_hbm, sgate),
                (sup_hbm, sup),
                (down_hbm, down),
                (sdown_hbm, sdown),
            )
        )
    ]
    for load in loads:
        load.start()
    loads[0].wait()

    def piece(c):
        start = c * chunk
        return pl.ds(start if isinstance(c, int) else pl.multiple_of(start, chunk), chunk)

    def gather(d, step, c, first=False, last=False):
        src = 0 if first or isinstance(step, int) and step == 1 else 2 * step - 3 + d
        dst = far if last else 2 * step - 1 + d
        return remote(
            xbuf.at[src, piece(c)],
            xbuf.at[dst, piece(c)],
            gs.at[d, step, c],
            gr.at[d, step, c],
            gather_to[d],
        )

    def gather_meta(d, step, first=False):
        src = 0 if first or isinstance(step, int) and step == 1 else 2 * step - 3 + d
        return remote(
            mbuf.at[src], mbuf.at[2 * step - 1 + d], ms.at[d, step], mr.at[d, step], gather_to[d]
        )

    def half(d):
        return range(CHUNKS // 2) if d == 0 else range(CHUNKS // 2, CHUNKS)

    def scaled(c):
        xbuf[0, piece(c)] = (tok[piece(c)].astype(F32) * gain_ref[...]).astype(BF16)

    for c in range(CHUNKS):
        scaled(c)
    pl.semaphore_wait(barrier, 2 + members - 1)
    for d in range(2):
        gather(d, 1, 0, first=True).start()

    def diagonal(c):
        shape = (chunk, count)
        return iota(shape, 0) + float(c * chunk) == iota(shape, 1)

    def squares_row(which, value_of):
        total = jnp.zeros((1, count), F32)
        for c in range(CHUNKS):
            value = value_of(c)
            column = jnp.sum(value * value, axis=1, keepdims=True)
            total = total + jnp.sum(
                jnp.where(diagonal(c), column, 0.0), axis=0, keepdims=True
            )
        squares[which, me] = jnp.broadcast_to(total, (8, count))

    def exchange_squares(which):
        copies = [
            remote(
                squares.at[which, me],
                squares.at[which, me],
                ns.at[which, d],
                nr.at[which, d],
                {"tp": lax.rem(me + d, members)},
            )
            for d in range(1, members)
        ]
        for copy in copies:
            copy.start()
        for copy in copies:
            copy.wait()
        total = squares[which, 0]
        for q in range(1, members):
            total = total + squares[which, q]
        return lax.rsqrt(total / features + epsilon)

    squares_row(0, lambda c: tok[piece(c)].astype(F32))
    mbuf[0, 0 : 2 * fanout] = meta_ref[...]
    mbuf[0, 2 * fanout :] = exchange_squares(0)
    for d in range(2):
        gather_meta(d, 1, first=True).start()
        for c in range(1, CHUNKS):
            gather(d, 1, c, first=True).start()

    square = (count, count)
    earlier[...] = jnp.where(iota(square, 0) < iota(square, 1), 1.0, 0.0).astype(BF16)
    eye[...] = jnp.where(iota(square, 0) == iota(square, 1), 1.0, 0.0).astype(BF16)

    def poll(step, c):
        for d in range(2):
            if c == 0:
                gather_meta(d, step).wait_recv()

                @pl.when(step + 1 < reach + 1 - d)
                def _():
                    gather_meta(d, step + 1).start()

            gather(d, step, c).wait_recv()

            @pl.when(step + 1 < reach)
            def _():
                gather(d, step + 1, c).start()

            if c in half(d):

                @pl.when(step + 1 == reach)
                def _():
                    gather(d, reach, c, last=True).start()

    def tables(k):
        first = (group * experts).astype(F32)
        wanted = first + iota((TABLE, count), 0)
        present = jnp.zeros((TABLE, count), F32)
        weight = jnp.zeros((TABLE, count), F32)
        for j in range(fanout):
            same = mbuf[k, j : j + 1] == wanted
            present = present + jnp.where(same, 1.0, 0.0)
            weight = weight + jnp.where(same, mbuf[k, fanout + j : fanout + j + 1], 0.0)
        slot = dot(present.astype(BF16), earlier[...])
        slotv[k] = jnp.where(present > 0.0, slot, -1.0)
        wv[k] = weight

    def row_values(at, size, hit, inverse, weight):
        inv = jnp.sum(jnp.where(hit, inverse, 0.0), axis=1, keepdims=True)
        rinv[at : at + size] = jnp.broadcast_to(inv, (size, 128))
        if weight is None:
            rwt[at : at + size] = jnp.ones((size, 128), F32)
        else:
            value = jnp.sum(jnp.where(hit, weight, 0.0), axis=1, keepdims=True)
            rwt[at : at + size] = jnp.broadcast_to(value, (size, 128))

    def put_parts(at, size, g, u):
        for q in range(members):
            parts[q, pl.ds(at, size), 0:share] = g[:, q * share : (q + 1) * share].astype(BF16)
            parts[q, pl.ds(at, size), share : 2 * share] = u[
                :, q * share : (q + 1) * share
            ].astype(BF16)

    def dispatch(blocks, shared):
        n = len(blocks)
        for i, k in enumerate(blocks):
            tables(k)
            inverse = mbuf[k, 2 * fanout : 2 * fanout + 1]
            for e in range(experts):
                hit = iota((cap, count), 0) == slotv[k, e : e + 1]
                hits[e * cap : (e + 1) * cap, 0:count] = jnp.where(hit, 1.0, 0.0).astype(BF16)
                row_values((e * n + i) * cap, cap, hit, inverse, wv[k, e : e + 1])

            def pick(j, carry):
                at = pl.ds(pl.multiple_of(j * COLUMNS, COLUMNS), COLUMNS)
                picked = dot(hits[0:slots, 0:count], xbuf[k, :, at]).astype(BF16)
                for e in range(experts):
                    rows[e, i * cap : (i + 1) * cap, at] = picked[e * cap : (e + 1) * cap]
                return carry

            lax.fori_loop(0, width // COLUMNS, pick, 0)

        def project(e, carry):
            taken = rows[e, 0 : n * cap]
            g, u = dot(taken, gate[e]), dot(taken, up[e])
            put_parts(pl.multiple_of(e * n * cap, n * cap), n * cap, g, u)
            return carry

        lax.fori_loop(0, experts, project, 0)
        if shared:
            inverse = mbuf[0, 2 * fanout : 2 * fanout + 1]
            for c in range(CHUNKS):
                row_values(slots + c * chunk, chunk, diagonal(c), inverse, None)

            def project_shared(c, carry):
                taken = xbuf[0, piece(c)]
                g, u = dot(taken, sgate[...]), dot(taken, sup[...])
                put_parts(pl.multiple_of(slots + c * chunk, 32), chunk, g, u)
                return carry

            lax.fori_loop(0, CHUNKS, project_shared, 0)

    def over_rows(total, body):
        size = 128 if total % 128 == 0 else total

        def run(j, carry):
            body(pl.ds(pl.multiple_of(j * size, size), size))
            return carry

        lax.fori_loop(0, total // size, run, 0)

    def core_copies(slot, total):
        return [
            remote(
                parts.at[y * 2 + 1 - core, pl.ds(0, total)],
                got1.at[slot, y, pl.ds(0, total)],
                s1s.at[slot, y],
                s1r.at[slot, y],
                partner,
            )
            for y in range(wide)
        ]

    def add_core(slot, total):
        def body(at):
            for y in range(wide):
                mine = parts[y * 2 + core, at].astype(F32)
                sums[y, at] = (mine + got1[slot, y, at].astype(F32)).astype(BF16)

        over_rows(total, body)

    def row_copies(total):
        return [
            remote(
                sums.at[peer_row(d), pl.ds(0, total)],
                got2.at[d - 1, pl.ds(0, total)],
                s2s.at[d],
                s2r.at[d],
                {"tp": peer_row(d) * 2 + core},
            )
            for d in range(1, wide)
        ]

    def activate(stage, total):
        def body(at):
            value = sums[row, at].astype(F32)
            for d in range(1, wide):
                value = value + got2[d - 1, at].astype(F32)
            inv = rinv[at, 0:share]
            g, u = value[:, 0:share] * inv, value[:, share : 2 * share] * inv
            hidden = g / (1.0 + jnp.exp(-g)) * u * rwt[at, 0:share]
            hid[stage, me, at] = hidden.astype(BF16)

        over_rows(total, body)

    def hidden_row_copies(stage, total):
        return [
            remote(
                hid.at[stage, me, pl.ds(0, total)],
                hid.at[stage, me, pl.ds(0, total)],
                s3s.at[d],
                s3r.at[d],
                {"tp": peer_row(d) * 2 + core},
            )
            for d in range(1, wide)
        ]

    def hidden_core_copies(stage, total):
        return [
            remote(
                hid.at[stage, y * 2 + core, pl.ds(0, total)],
                hid.at[stage, y * 2 + core, pl.ds(0, total)],
                s4s.at[lax.rem(stage, 2), y],
                s4r.at[lax.rem(stage, 2), y],
                partner,
            )
            for y in range(wide)
        ]

    def start(copies):
        for copy in copies:
            copy.start()

    def wait(copies):
        for copy in copies:
            copy.wait()

    def combine(stage, blocks, put):
        n = len(blocks)

        def produce(e, carry):
            at = pl.ds(pl.multiple_of(e * n * cap, n * cap), n * cap)
            taken = jnp.concatenate([hid[stage, q, at] for q in range(members)], axis=1)
            result = dot(taken, down[e]).astype(BF16)
            for i in range(n):
                made[i, pl.ds(pl.multiple_of(e * cap, cap), cap)] = result[i * cap : (i + 1) * cap]
            return carry

        lax.fori_loop(0, experts, produce, 0)
        for i, k in enumerate(blocks):
            slot_column = dot_nt(eye[...], slotv[k].astype(BF16))
            for e in range(experts):
                hit = iota((count, cap), 1) == slot_column[:, e : e + 1]
                hits[0:count, e * cap : (e + 1) * cap] = jnp.where(hit, 1.0, 0.0).astype(BF16)

            def tile(j, carry):
                at = pl.ds(pl.multiple_of(j * COLUMNS, COLUMNS), COLUMNS)
                put(i, at, dot(hits[0:count, 0:slots], made[i, :, at]))
                return carry

            lax.fori_loop(0, width // COLUMNS, tile, 0)

    first_rows = slots + count
    pair_rows = 2 * slots

    for i in range(1, 5):
        loads[i].wait()
    dispatch([0], True)
    start(core_copies(0, first_rows))
    poll(1, 0)
    wait(core_copies(0, first_rows))
    add_core(0, first_rows)
    start(row_copies(first_rows))
    poll(1, 1)
    poll(1, 2)
    wait(row_copies(first_rows))
    activate(0, first_rows)
    start(hidden_row_copies(0, first_rows))
    poll(1, 3)

    def before(s, total_before):
        wait(hidden_row_copies(s - 1, total_before))
        start(hidden_core_copies(s - 1, total_before))

    def run_stage(s, carry):
        @pl.when(s == 2)
        def _():
            wait(hidden_core_copies(0, first_rows))

        @pl.when(s > 2)
        def _():
            wait(hidden_core_copies(s - 2, pair_rows))

        dispatch([2 * s - 1, 2 * s], False)
        slot = lax.rem(s, 2)
        start(core_copies(slot, pair_rows))

        def more(c):
            @pl.when(s + 1 < reach)
            def _():
                poll(s + 1, c)

        more(0)
        wait(core_copies(slot, pair_rows))
        add_core(slot, pair_rows)

        @pl.when(s == 1)
        def _():
            before(1, first_rows)

        @pl.when(s > 1)
        def _():
            before(s, pair_rows)

        start(row_copies(pair_rows))
        more(1)
        more(2)
        wait(row_copies(pair_rows))
        activate(s, pair_rows)
        start(hidden_row_copies(s, pair_rows))
        more(3)
        return carry

    lax.fori_loop(1, reach, run_stage, 0)

    wait(hidden_core_copies(reach - 2, pair_rows if reach > 2 else first_rows))
    gather_meta(0, reach).wait_recv()
    for d in range(2):
        for c in half(d):
            gather(d, reach, c, last=True).wait_recv()
    dispatch([far], False)
    start(core_copies(reach % 2, slots))

    def sent(step, carry):
        for d in range(2):
            for c in range(CHUNKS):
                gather(d, step, c).wait_send()
            gather_meta(d, step).wait_send()
        return carry

    for d in range(2):
        for c in range(CHUNKS):
            gather(d, 1, c, first=True).wait_send()
        gather_meta(d, 1, first=True).wait_send()
        for c in half(d):
            gather(d, reach, c, last=True).wait_send()
    lax.fori_loop(2, reach, sent, 0)
    gather_meta(0, reach).wait_send()
    pl.semaphore_signal(credit.at[1], inc=1, device_id=return_to[0], device_id_type=MESH)
    pl.semaphore_signal(credit.at[0], inc=1, device_id=return_to[1], device_id_type=MESH)

    wait(core_copies(reach % 2, slots))
    add_core(reach % 2, slots)
    before(reach, pair_rows)
    start(row_copies(slots))
    wait(hidden_core_copies(reach - 1, pair_rows))

    def give(d, step, c, source):
        return remote(
            source.at[piece(c)],
            xbuf.at[2 * step - 1 + d, piece(c)],
            rs.at[d, step, c],
            rr.at[d, step, c],
            return_to[d],
        )

    def ready(s):
        def put(i, at, value):
            back[s % 2 if isinstance(s, int) else lax.rem(s, 2), i, :, at] = value.astype(BF16)

        combine(s, [2 * s - 1, 2 * s], put)

    loads[5].wait()
    ready(reach - 1)
    top = back.at[(reach - 1) % 2]
    for d in range(2):
        pl.semaphore_wait(credit.at[d], 1)
    order = [list(half(1)) + list(half(0)), list(half(0)) + list(half(1))]
    for j in range(CHUNKS // 2):
        for d in range(2):
            c = order[d][j]
            give(d, 2, c, top.at[d]).start()

    wait(row_copies(slots))
    activate(reach, slots)
    start(hidden_row_copies(reach, slots))
    wait(hidden_row_copies(reach, slots))
    start(hidden_core_copies(reach, slots))
    wait(hidden_core_copies(reach, slots))

    def put_far(i, at, value):
        farb[:, at] = value.astype(BF16)

    combine(reach, [far], put_far)
    for j in range(CHUNKS // 2):
        for d in range(2):
            c = order[d][CHUNKS // 2 + j]
            give(d, 1, c, farb).start()
    if reach > 2:
        ready(reach - 2)

    def merge(d, step, c, source):
        give(d, step - 1, c, source).wait_recv()
        own = source[piece(c)].astype(F32)
        source[piece(c)] = (own + xbuf[2 * step - 3 + d, piece(c)].astype(F32)).astype(BF16)
        give(d, step, c, source).start()

    for j in range(CHUNKS // 2):
        for d in range(2):
            merge(d, 2, order[d][CHUNKS // 2 + j], top.at[d])

    for d in range(2):
        for c in half(d):
            give(d, 1, c, farb).wait_send()

    def returning(step, carry):
        s = reach + 1 - step
        now = back.at[lax.rem(s, 2)]
        for j in range(CHUNKS):
            for d in range(2):
                merge(d, step, order[d][j], now.at[d])
        for d in range(2):
            for c in range(CHUNKS):
                give(d, step - 1, c, back.at[lax.rem(s + 1, 2), d]).wait_send()

        @pl.when(s > 1)
        def _():
            ready(s - 1)

        return carry

    lax.fori_loop(3, reach + 1, returning, 0)

    loads[6].wait()

    def put_own(i, at, value):
        taken = jnp.concatenate(
            [hid[0, q, slots : slots + count] for q in range(members)], axis=1
        )
        mix[:, at] = value + dot(taken, sdown[:, at])

    combine(0, [0], put_own)
    for d in range(2):
        for c in range(CHUNKS):
            give(d, reach, c, back.at[1, d]).wait_send()
    for j in range(CHUNKS):
        for d in range(2):
            c = order[d][j]
            give(d, reach, c, back.at[1, d]).wait_recv()
            mix[piece(c)] = mix[piece(c)] + xbuf[2 * reach - 1 + d, piece(c)].astype(F32)
    squares_row(1, lambda c: mix[piece(c)])
    scale = exchange_squares(1)[0:1]
    for c in range(CHUNKS):
        column = jnp.sum(jnp.where(diagonal(c), scale, 0.0), axis=1, keepdims=True)
        out_ref[piece(c)] = (mix[piece(c)] * column * post_ref[...]).astype(BF16)


def per_device(
    tokens,
    routes,
    route_weights,
    pre_gain,
    expert_gate,
    expert_up,
    expert_down,
    shared_gate,
    shared_up,
    shared_down,
    post_gain,
):
    members, groups = lax.axis_size("tp"), lax.axis_size("ep")
    count, width = tokens.shape
    fanout = routes.shape[1]
    experts, _, units = expert_gate.shape
    cap = 2 * count * fanout // (experts * groups)
    ring = tuple(ring_of(groups, members // 2))
    reach, wide = groups // 2, members // 2
    slots = experts * cap
    most = max(2 * slots, slots + count)
    share = units // members
    meta = jnp.concatenate([routes.astype(F32), route_weights], axis=1).T
    cfg = (groups, members, experts, cap, fanout, ring, float(width * members))

    vmem = pl.BlockSpec(memory_space=pltpu.VMEM)
    anywhere = pl.BlockSpec(memory_space=pl.ANY)
    dma = pltpu.SemaphoreType.DMA
    steps = reach + 1
    return pl.pallas_call(
        functools.partial(layer_kernel, cfg),
        out_shape=jax.ShapeDtypeStruct((count, width), BF16),
        in_specs=[anywhere, vmem, vmem] + [anywhere] * 6 + [vmem],
        out_specs=vmem,
        scratch_shapes=[
            pltpu.VMEM((count, width), BF16),
            pltpu.VMEM((groups + 1, count, width), BF16),
            pltpu.VMEM((groups, 2 * fanout + 8, count), F32),
            pltpu.VMEM(expert_gate.shape, BF16),
            pltpu.VMEM(expert_up.shape, BF16),
            pltpu.VMEM(expert_down.shape, BF16),
            pltpu.VMEM(shared_gate.shape, BF16),
            pltpu.VMEM(shared_up.shape, BF16),
            pltpu.VMEM(shared_down.shape, BF16),
            pltpu.VMEM((experts, 2 * cap, width), BF16),
            pltpu.VMEM((max(slots, count), max(slots, count)), BF16),
            pltpu.VMEM((members, most, 2 * share), BF16),
            pltpu.VMEM((2, wide, most, 2 * share), BF16),
            pltpu.VMEM((wide, most, 2 * share), BF16),
            pltpu.VMEM((wide - 1, most, 2 * share), BF16),
            pltpu.VMEM((reach + 1, members, most, share), BF16),
            pltpu.VMEM((2, slots, width), BF16),
            pltpu.VMEM((2, 2, count, width), BF16),
            pltpu.VMEM((count, width), BF16),
            pltpu.VMEM((count, width), F32),
            pltpu.VMEM((groups, TABLE, count), F32),
            pltpu.VMEM((groups, TABLE, count), F32),
            pltpu.VMEM((most, 128), F32),
            pltpu.VMEM((most, 128), F32),
            pltpu.VMEM((count, count), BF16),
            pltpu.VMEM((count, count), BF16),
            pltpu.VMEM((2, members, 8, count), F32),
            dma((7,)),
            dma((2, steps, CHUNKS)),
            dma((2, steps, CHUNKS)),
            dma((2, steps)),
            dma((2, steps)),
            dma((2, steps, CHUNKS)),
            dma((2, steps, CHUNKS)),
            dma((2, wide)),
            dma((2, wide)),
            dma((wide,)),
            dma((wide,)),
            dma((wide,)),
            dma((wide,)),
            dma((2, wide)),
            dma((2, wide)),
            dma((2, members)),
            dma((2, members)),
            pltpu.SemaphoreType.REGULAR((2,)),
        ],
        compiler_params=pltpu.CompilerParams(
            collective_id=0, has_side_effects=True, vmem_limit_bytes=67043328
        ),
        name="layer",
    )(
        tokens,
        meta,
        pre_gain[None, :],
        expert_gate,
        expert_up,
        expert_down,
        shared_gate,
        shared_up,
        shared_down,
        post_gain[None, :],
    )


def solution(mesh):
    in_specs = (
        P("ep", "tp"),
        P("ep", None),
        P("ep", None),
        P("tp"),
        P("ep", "tp", None),
        P("ep", "tp", None),
        P("ep", None, "tp"),
        P("tp", None),
        P("tp", None),
        P(None, "tp"),
        P("tp"),
    )
    return jax.shard_map(
        per_device, mesh=mesh, in_specs=in_specs, out_specs=P("ep", "tp"), check_vma=False
    )
```

```python
import functools

import jax
import jax.numpy as jnp
from jax import lax
from jax.experimental import pallas as pl
from jax.experimental.pallas import tpu as pltpu
from jax.sharding import PartitionSpec as P

epsilon = 1e-06
MESH = pl.DeviceIdType.MESH
F32, BF16 = jnp.float32, jnp.bfloat16
CHUNKS = 4
TABLE = 16
COLUMNS = 256


def ring_of(groups, width):
    if width < 2 or groups % width or groups // width < 2:
        return list(range(groups))
    depth = groups // width
    cycle = []
    for x in range(width):
        column = range(1, depth) if x % 2 == 0 else range(depth - 1, 0, -1)
        cycle += [z * width + x for z in column]
    return cycle + [x for x in range(width - 1, -1, -1)]


def dot(a, b):
    return jnp.dot(a, b, preferred_element_type=F32)


def dot_nt(a, b):
    return lax.dot_general(a, b, (((1,), (1,)), ((), ())), preferred_element_type=F32)


def iota(shape, axis):
    return lax.broadcasted_iota(jnp.int32, shape, axis).astype(F32)


def layer_kernel(
    cfg,
    tokens_hbm,
    routes_ref,
    weights_ref,
    gain_ref,
    gate_hbm,
    up_hbm,
    down_hbm,
    sgate_hbm,
    sup_hbm,
    sdown_hbm,
    post_ref,
    out_ref,
    tok,
    xbuf,
    mbuf,
    gate,
    up,
    down,
    sgate,
    sup,
    sdown,
    rows,
    hits,
    lifts,
    parts,
    got1,
    sums,
    got2,
    hid,
    made,
    back,
    farb,
    mix,
    slotv,
    wv,
    rinv,
    rwt,
    earlier,
    eye,
    squares,
    token_sem,
    load_sem,
    gs,
    gr,
    ms,
    mr,
    rs,
    rr,
    s1s,
    s1r,
    s2s,
    s2r,
    s3s,
    s3r,
    s4s,
    s4r,
    ns,
    nr,
    credit,
):
    groups, members, experts, cap, fanout, ring, features = cfg
    count, width = out_ref.shape
    reach = groups // 2
    wide = members // 2
    units = gate.shape[2]
    share = units // members
    chunk = count // CHUNKS
    slots = experts * cap
    far = 2 * reach - 1
    middle = count // 2
    packed = mbuf.shape[1]

    group, me = lax.axis_index("ep"), lax.axis_index("tp")
    core, row = lax.rem(me, 2), lax.div(me, 2)
    ahead, behind = jnp.int32(0), jnp.int32(0)
    for i, place in enumerate(ring):
        here = group == place
        ahead = jnp.where(here, ring[(i + 1) % groups], ahead)
        behind = jnp.where(here, ring[(i - 1) % groups], behind)
    gather_to = ({"ep": ahead}, {"ep": behind})
    return_to = ({"ep": behind}, {"ep": ahead})
    partner = {"tp": row * 2 + 1 - core}

    def peer_row(d):
        return lax.rem(row + d, wide)

    def remote(src, dst, send, recv, to):
        return pltpu.make_async_remote_copy(
            src_ref=src, dst_ref=dst, send_sem=send, recv_sem=recv, device_id=to, device_id_type=MESH
        )

    barrier = pltpu.get_barrier_semaphore()
    for to in gather_to:
        pl.semaphore_signal(barrier, inc=1, device_id=to, device_id_type=MESH)
    for d in range(1, members):
        pl.semaphore_signal(
            barrier, inc=1, device_id={"tp": lax.rem(me + d, members)}, device_id_type=MESH
        )

    def piece(c):
        at = c * chunk
        return pl.ds(at if isinstance(c, int) else pl.multiple_of(at, chunk), chunk)

    token_loads = [
        pltpu.make_async_copy(tokens_hbm.at[piece(c)], tok.at[piece(c)], token_sem.at[c])
        for c in range(CHUNKS)
    ]
    for load in token_loads:
        load.start()
    loads = [
        pltpu.make_async_copy(src, dst, load_sem.at[i])
        for i, (src, dst) in enumerate(
            (
                (gate_hbm, gate),
                (up_hbm, up),
                (sgate_hbm, sgate),
                (sup_hbm, sup),
                (down_hbm, down),
                (sdown_hbm, sdown),
            )
        )
    ]

    def gather(d, step, c, first=False, last=False):
        src = 0 if first or isinstance(step, int) and step == 1 else 2 * step - 3 + d
        dst = far if last else 2 * step - 1 + d
        return remote(
            xbuf.at[src, piece(c)],
            xbuf.at[dst, piece(c)],
            gs.at[d, step, c],
            gr.at[d, step, c],
            gather_to[d],
        )

    def gather_meta(d, step, first=False):
        src = 0 if first or isinstance(step, int) and step == 1 else 2 * step - 3 + d
        return remote(
            mbuf.at[src], mbuf.at[2 * step - 1 + d], ms.at[d, step], mr.at[d, step], gather_to[d]
        )

    def half(d):
        return range(CHUNKS // 2) if d == 0 else range(CHUNKS // 2, CHUNKS)

    def scaled(c):
        xbuf[0, piece(c)] = (tok[piece(c)].astype(F32) * gain_ref[...]).astype(BF16)

    def diagonal(c):
        shape = (chunk, count)
        return iota(shape, 0) + float(c * chunk) == iota(shape, 1)

    def squares_of(c, value):
        column = jnp.sum(value * value, axis=1, keepdims=True)
        return jnp.sum(jnp.where(diagonal(c), column, 0.0), axis=0, keepdims=True)

    token_loads[0].wait()
    scaled(0)
    pl.semaphore_wait(barrier, 2 + members - 1)
    for d in range(2):
        gather(d, 1, 0, first=True).start()
    for c in range(1, CHUNKS):
        token_loads[c].wait()
    for load in loads:
        load.start()
    own_squares = jnp.zeros((1, count), F32)
    for c in range(CHUNKS):
        own_squares = own_squares + squares_of(c, tok[piece(c)].astype(F32))
    squares[0, me] = jnp.broadcast_to(own_squares, (8, count))

    def exchange_squares(which, meanwhile=lambda: None):
        copies = [
            remote(
                squares.at[which, me],
                squares.at[which, me],
                ns.at[which, d],
                nr.at[which, d],
                {"tp": lax.rem(me + d, members)},
            )
            for d in range(1, members)
        ]
        for copy in copies:
            copy.start()
        meanwhile()
        for copy in copies:
            copy.wait()
        total = squares[which, 0]
        for q in range(1, members):
            total = total + squares[which, q]
        return lax.rsqrt(total / features + epsilon)

    def finish_tokens():
        for c in range(1, CHUNKS):
            scaled(c)
        earlier[...] = jnp.where(iota(square, 0) < iota(square, 1), 1.0, 0.0).astype(BF16)
        eye[...] = jnp.where(iota(square, 0) == iota(square, 1), 1.0, 0.0).astype(BF16)

    square = (count, count)
    inverse_row = exchange_squares(0, finish_tokens)[0:1]
    high_weight = weights_ref[...].astype(BF16).astype(F32)
    high = inverse_row.astype(BF16).astype(F32)
    mid = (inverse_row - high).astype(BF16).astype(F32)
    mbuf[0] = jnp.concatenate(
        [
            routes_ref[...].astype(F32),
            high_weight,
            weights_ref[...] - high_weight,
            high,
            mid,
            inverse_row - high - mid,
        ]
        + [jnp.zeros((packed - 3 * fanout - 3, count), F32)],
        axis=0,
    ).astype(BF16)
    for d in range(2):
        gather_meta(d, 1, first=True).start()
        for c in range(1, CHUNKS):
            gather(d, 1, c, first=True).start()

    def poll(step, c):
        for d in range(2):
            if c == 0:
                gather_meta(d, step).wait_recv()

                @pl.when(step + 1 < reach + 1 - d)
                def _():
                    gather_meta(d, step + 1).start()

            gather(d, step, c).wait_recv()

            @pl.when(step + 1 < reach)
            def _():
                gather(d, step + 1, c).start()

            if c in half(d):

                @pl.when(step + 1 == reach)
                def _():
                    gather(d, reach, c, last=True).start()

    def tables(k):
        first = (group * experts).astype(F32)
        wanted = first + iota((TABLE, count), 0)
        present = jnp.zeros((TABLE, count), F32)
        weight = jnp.zeros((TABLE, count), F32)
        values = mbuf[k].astype(F32)
        for j in range(fanout):
            same = values[j : j + 1] == wanted
            present = present + jnp.where(same, 1.0, 0.0)
            exact = values[fanout + j : fanout + j + 1] + values[2 * fanout + j : 2 * fanout + j + 1]
            weight = weight + jnp.where(same, exact, 0.0)
        slot = dot(present.astype(BF16), earlier[...])
        slotv[k] = jnp.where(present > 0.0, slot, -1.0)
        wv[k] = weight
        at = 3 * fanout
        return values[at : at + 1] + values[at + 1 : at + 2] + values[at + 2 : at + 3]

    def row_values(turn, at, size, hit, inverse, weight):
        inv = jnp.sum(jnp.where(hit, inverse, 0.0), axis=1, keepdims=True)
        rinv[turn, at : at + size] = jnp.broadcast_to(inv, (size, 128))
        if weight is None:
            rwt[turn, at : at + size] = jnp.ones((size, 128), F32)
        else:
            value = jnp.sum(jnp.where(hit, weight, 0.0), axis=1, keepdims=True)
            rwt[turn, at : at + size] = jnp.broadcast_to(value, (size, 128))

    def prepare(turn, blocks, shared=False):
        n = len(blocks)
        for i, k in enumerate(blocks):
            inverse = tables(k)
            for e in range(experts):
                hit = iota((cap, count), 0) == slotv[k, e : e + 1]
                hits[i, e * cap : (e + 1) * cap] = jnp.where(hit, 1.0, 0.0).astype(BF16)
                row_values(turn, (e * n + i) * cap, cap, hit, inverse, wv[k, e : e + 1])
        if shared:
            for c in range(CHUNKS):
                row_values(turn, slots + c * chunk, chunk, diagonal(c), inverse, None)

    def put_parts(at, size, g, u):
        for q in range(members):
            parts[q, pl.ds(at, size), 0:share] = g[:, q * share : (q + 1) * share].astype(BF16)
            parts[q, pl.ds(at, size), share : 2 * share] = u[
                :, q * share : (q + 1) * share
            ].astype(BF16)

    def pick_rows(blocks, part=None):
        low, high = (0, count) if part is None else (part * middle, (part + 1) * middle)
        for i, k in enumerate(blocks):

            def pick(j, carry):
                at = pl.ds(pl.multiple_of(j * COLUMNS, COLUMNS), COLUMNS)
                picked = dot(hits[i, :, low:high], xbuf[k, low:high, at]).astype(BF16)
                for e in range(experts):
                    value = picked[e * cap : (e + 1) * cap]
                    if part == 1:
                        value = value + rows[e, i * cap : (i + 1) * cap, at]
                    rows[e, i * cap : (i + 1) * cap, at] = value
                return carry

            lax.fori_loop(0, width // COLUMNS, pick, 0)

    def project(e, n):
        taken = rows[e, 0 : n * cap]
        g, u = dot(taken, gate[e]), dot(taken, up[e])
        put_parts(pl.multiple_of(e * n * cap, n * cap), n * cap, g, u)

    def span(k, total):
        size = total // experts
        return pl.ds(k * size if isinstance(k, int) else pl.multiple_of(k * size, size), size)

    def core_copies(turn, k, total):
        return [
            remote(
                parts.at[y * 2 + 1 - core, span(k, total)],
                got1.at[turn, y, span(k, total)],
                s1s.at[turn, k, y],
                s1r.at[turn, k, y],
                partner,
            )
            for y in range(wide)
        ]

    def row_copies(turn, k, total):
        return [
            remote(
                sums.at[peer_row(d), span(k, total)],
                got2.at[turn, d - 1, span(k, total)],
                s2s.at[turn, k, d],
                s2r.at[turn, k, d],
                {"tp": peer_row(d) * 2 + core},
            )
            for d in range(1, wide)
        ]

    def hidden_row_copies(stage, k, total):
        turn = lax.rem(stage, 2)
        return [
            remote(
                hid.at[stage, me, span(k, total)],
                hid.at[stage, me, span(k, total)],
                s3s.at[turn, k, d],
                s3r.at[turn, k, d],
                {"tp": peer_row(d) * 2 + core},
            )
            for d in range(1, wide)
        ]

    def hidden_core_copies(stage, k, total):
        turn = lax.rem(stage, 2)
        return [
            remote(
                hid.at[stage, y * 2 + core, span(k, total)],
                hid.at[stage, y * 2 + core, span(k, total)],
                s4s.at[turn, k, y],
                s4r.at[turn, k, y],
                partner,
            )
            for y in range(wide)
        ]

    def start(copies):
        for copy in copies:
            copy.start()

    def wait(copies):
        for copy in copies:
            copy.wait()

    def add_core(turn, k, total):
        wait(core_copies(turn, k, total))
        at = span(k, total)
        for y in range(wide):
            mine = parts[y * 2 + core, at].astype(F32)
            sums[y, at] = (mine + got1[turn, y, at].astype(F32)).astype(BF16)
        start(row_copies(turn, k, total))

    def activate(stage, turn, k, total):
        wait(row_copies(turn, k, total))
        at = span(k, total)
        value = sums[row, at].astype(F32)
        for d in range(1, wide):
            value = value + got2[turn, d - 1, at].astype(F32)
        inv = rinv[turn, at, 0:share]
        g, u = value[:, 0:share] * inv, value[:, share : 2 * share] * inv
        hidden = g / (1.0 + jnp.exp(-g)) * u * rwt[turn, at, 0:share]
        hid[stage, me, at] = hidden.astype(BF16)
        start(hidden_row_copies(stage, k, total))

    def pass_hidden(stage, total):
        for k in range(experts):
            wait(hidden_row_copies(stage, k, total))
            start(hidden_core_copies(stage, k, total))

    def take_hidden(stage, total):
        for k in range(experts):
            wait(hidden_core_copies(stage, k, total))

    def send_parts(turn, n, total):
        def body(e, carry):
            project(e, n)
            start(core_copies(turn, e, total))

            @pl.when(e > 0)
            def _():
                add_core(turn, e - 1, total)

            return carry

        lax.fori_loop(0, experts, body, 0)
        add_core(turn, experts - 1, total)

    def columns(at, k):
        slot_column = dot_nt(eye[...], slotv[k].astype(BF16))
        for e in range(experts):
            hit = iota((count, cap), 1) == slot_column[:, e : e + 1]
            lifts[at, :, e * cap : (e + 1) * cap] = jnp.where(hit, 1.0, 0.0).astype(BF16)

    def produce(stage, e, n, first):
        at = pl.ds(pl.multiple_of(e * n * cap, n * cap), n * cap)
        taken = jnp.concatenate([hid[stage, q, at] for q in range(members)], axis=1)
        result = dot(taken, down[e]).astype(BF16)
        for i in range(n):
            made[first + i, pl.ds(pl.multiple_of(e * cap, cap), cap)] = result[
                i * cap : (i + 1) * cap
            ]

    def produce_all(stage, n, first):
        def body(e, carry):
            produce(stage, e, n, first)
            return carry

        lax.fori_loop(0, experts, body, 0)

    def scatter(i, low, high, put):
        def tile(j, carry):
            at = pl.ds(pl.multiple_of(j * COLUMNS, COLUMNS), COLUMNS)
            put(at, dot(lifts[i, low:high], made[i, :, at]))
            return carry

        lax.fori_loop(0, width // COLUMNS, tile, 0)

    first_rows = slots + count
    pair_rows = 2 * slots

    prepare(0, [0], True)
    for i in range(4):
        loads[i].wait()
    pick_rows([0])

    def own_rows(e, carry):
        project(e, 1)
        return carry

    lax.fori_loop(0, experts, own_rows, 0)

    def shared_rows(c, carry):
        taken = xbuf[0, piece(c)]
        g, u = dot(taken, sgate[...]), dot(taken, sup[...])
        put_parts(pl.multiple_of(slots + c * chunk, 32), chunk, g, u)
        return carry

    lax.fori_loop(0, CHUNKS, shared_rows, 0)
    for k in range(experts):
        start(core_copies(0, k, first_rows))
    for k in range(experts):
        add_core(0, k, first_rows)
    poll(1, 0)
    prepare(1, [1, 2])
    for k in range(experts):
        activate(0, 0, k, first_rows)
        if k == 0:
            poll(1, 1)
            pick_rows([1, 2], 0)
        if k == experts - 2:
            poll(1, 2)
    poll(1, 3)

    def run_stage(s, carry):
        turn = lax.rem(s, 2)

        @pl.when(s == 2)
        def _():
            take_hidden(0, first_rows)

        @pl.when(s > 2)
        def _():
            take_hidden(s - 2, pair_rows)

        pick_rows([2 * s - 1, 2 * s], 1)
        send_parts(turn, 2, pair_rows)
        @pl.when(s == 1)
        def _():
            pass_hidden(0, first_rows)

        @pl.when(s > 1)
        def _():
            pass_hidden(s - 1, pair_rows)

        def more(c):
            @pl.when(s + 1 < reach)
            def _():
                poll(s + 1, c)

        more(0)

        @pl.when(s + 1 < reach)
        def _():
            prepare(1 - turn, [2 * s + 1, 2 * s + 2])

        @pl.when(s + 1 == reach)
        def _():
            gather_meta(0, reach).wait_recv()
            prepare(1 - turn, [far])

        for k in range(experts):
            activate(s, turn, k, pair_rows)
            if k == 0:
                more(1)

                @pl.when(s + 1 < reach)
                def _():
                    pick_rows([2 * s + 1, 2 * s + 2], 0)

            if k == experts - 2:
                more(2)
        more(3)
        return carry

    lax.fori_loop(1, reach, run_stage, 0)

    last, spare = reach - 1, reach % 2
    take_hidden(reach - 2, pair_rows if reach > 2 else first_rows)
    for d in range(2):
        for c in half(d):
            gather(d, reach, c, last=True).wait_recv()
    pick_rows([far])
    send_parts(spare, 1, slots)
    columns(0, 2 * last - 1)
    columns(1, 2 * last)
    loads[4].wait()
    for k in range(experts):
        wait(hidden_row_copies(last, k, pair_rows))
        start(hidden_core_copies(last, k, pair_rows))
        if k > 0:
            wait(hidden_core_copies(last, k - 1, pair_rows))
            produce(last, k - 1, 2, 0)

    def sent(step, carry):
        for d in range(2):
            for c in range(CHUNKS):
                gather(d, step, c).wait_send()
            gather_meta(d, step).wait_send()
        return carry

    for d in range(2):
        for c in range(CHUNKS):
            gather(d, 1, c, first=True).wait_send()
        gather_meta(d, 1, first=True).wait_send()
        for c in half(d):
            gather(d, reach, c, last=True).wait_send()
    lax.fori_loop(2, reach, sent, 0)
    gather_meta(0, reach).wait_send()
    pl.semaphore_signal(credit.at[1], inc=1, device_id=return_to[0], device_id_type=MESH)
    pl.semaphore_signal(credit.at[0], inc=1, device_id=return_to[1], device_id_type=MESH)
    wait(hidden_core_copies(last, experts - 1, pair_rows))
    produce(last, experts - 1, 2, 0)

    def give(d, step, c, source):
        return remote(
            source.at[piece(c)],
            xbuf.at[2 * step - 1 + d, piece(c)],
            rs.at[d, step, c],
            rr.at[d, step, c],
            return_to[d],
        )

    def into(side, i, low, high):
        def put(at, value):
            back[side, i, low:high, at] = value.astype(BF16)

        return put

    side = last % 2
    top = back.at[side]
    order = [list(half(1)) + list(half(0)), list(half(0)) + list(half(1))]
    for d in range(2):
        low = middle if d == 0 else 0
        scatter(d, low, low + middle, into(side, d, low, low + middle))
        pl.semaphore_wait(credit.at[d], 1)
        for j in range(CHUNKS // 2):
            give(d, 2, order[d][j], top.at[d]).start()

    for k in range(experts):
        activate(reach, spare, k, slots)
    columns(2, far)
    for d in range(2):
        low = 0 if d == 0 else middle
        scatter(d, low, low + middle, into(side, d, low, low + middle))
    for k in range(experts):
        wait(hidden_row_copies(reach, k, slots))
        start(hidden_core_copies(reach, k, slots))
        if k > 0:
            wait(hidden_core_copies(reach, k - 1, slots))
            produce(reach, k - 1, 1, 2)
    wait(hidden_core_copies(reach, experts - 1, slots))
    produce(reach, experts - 1, 1, 2)

    def put_far(at, value):
        farb[:, at] = value.astype(BF16)

    scatter(2, 0, count, put_far)
    for j in range(CHUNKS // 2):
        for d in range(2):
            give(d, 1, order[d][CHUNKS // 2 + j], farb).start()

    def ready(s):
        produce_all(s, 2, 0)
        for i in range(2):
            columns(i, 2 * s - 1 + i)
            scatter(i, 0, count, into(lax.rem(s, 2), i, 0, count))

    if reach > 2:
        ready(reach - 2)

    def merge(d, step, c, source):
        give(d, step - 1, c, source).wait_recv()
        own = source[piece(c)].astype(F32)
        source[piece(c)] = (own + xbuf[2 * step - 3 + d, piece(c)].astype(F32)).astype(BF16)
        give(d, step, c, source).start()

    for j in range(CHUNKS // 2):
        for d in range(2):
            merge(d, 2, order[d][CHUNKS // 2 + j], top.at[d])

    for d in range(2):
        for c in half(d):
            give(d, 1, c, farb).wait_send()

    def returning(step, carry):
        s = reach + 1 - step
        now = back.at[lax.rem(s, 2)]
        for j in range(CHUNKS):
            for d in range(2):
                merge(d, step, order[d][j], now.at[d])
        for d in range(2):
            for c in range(CHUNKS):
                give(d, step - 1, c, back.at[lax.rem(s + 1, 2), d]).wait_send()

        @pl.when(s > 1)
        def _():
            ready(s - 1)

        return carry

    lax.fori_loop(3, reach + 1, returning, 0)

    loads[5].wait()

    def put_own(at, value):
        taken = jnp.concatenate(
            [hid[0, q, slots : slots + count] for q in range(members)], axis=1
        )
        mix[:, at] = value + dot(taken, sdown[:, at])

    produce_all(0, 1, 0)
    columns(0, 0)
    scatter(0, 0, count, put_own)
    taken_chunks = [0] * CHUNKS
    total = jnp.zeros((1, count), F32)
    for j in range(CHUNKS):
        for d in range(2):
            c = order[d][j]
            give(d, reach, c, back.at[1, d]).wait_recv()
            value = mix[piece(c)] + xbuf[2 * reach - 1 + d, piece(c)].astype(F32)
            mix[piece(c)] = value
            taken_chunks[c] += 1
            if taken_chunks[c] == 2:
                total = total + squares_of(c, value)
    squares[1, me] = jnp.broadcast_to(total, (8, count))
    scale = exchange_squares(1)[0:1]
    for c in range(CHUNKS):
        column = jnp.sum(jnp.where(diagonal(c), scale, 0.0), axis=1, keepdims=True)
        out_ref[piece(c)] = (mix[piece(c)] * column * post_ref[...]).astype(BF16)
    for d in range(2):
        for c in range(CHUNKS):
            give(d, reach, c, back.at[1, d]).wait_send()


def per_device(
    tokens,
    routes,
    route_weights,
    pre_gain,
    expert_gate,
    expert_up,
    expert_down,
    shared_gate,
    shared_up,
    shared_down,
    post_gain,
):
    members, groups = lax.axis_size("tp"), lax.axis_size("ep")
    count, width = tokens.shape
    fanout = routes.shape[1]
    experts, _, units = expert_gate.shape
    cap = 2 * count * fanout // (experts * groups)
    ring = tuple(ring_of(groups, members // 2))
    reach, wide = groups // 2, members // 2
    slots = experts * cap
    most = max(2 * slots, slots + count)
    share = units // members
    cfg = (groups, members, experts, cap, fanout, ring, float(width * members))

    vmem = pl.BlockSpec(memory_space=pltpu.VMEM)
    anywhere = pl.BlockSpec(memory_space=pl.ANY)
    dma = pltpu.SemaphoreType.DMA
    steps = reach + 1
    return pl.pallas_call(
        functools.partial(layer_kernel, cfg),
        out_shape=jax.ShapeDtypeStruct((count, width), BF16),
        in_specs=[anywhere, vmem, vmem, vmem] + [anywhere] * 6 + [vmem],
        out_specs=vmem,
        scratch_shapes=[
            pltpu.VMEM((count, width), BF16),
            pltpu.VMEM((groups + 1, count, width), BF16),
            pltpu.VMEM((groups, -(-(3 * fanout + 3) // 16) * 16, count), BF16),
            pltpu.VMEM(expert_gate.shape, BF16),
            pltpu.VMEM(expert_up.shape, BF16),
            pltpu.VMEM(expert_down.shape, BF16),
            pltpu.VMEM(shared_gate.shape, BF16),
            pltpu.VMEM(shared_up.shape, BF16),
            pltpu.VMEM(shared_down.shape, BF16),
            pltpu.VMEM((experts, 2 * cap, width), BF16),
            pltpu.VMEM((2, slots, count), BF16),
            pltpu.VMEM((3, count, slots), BF16),
            pltpu.VMEM((members, most, 2 * share), BF16),
            pltpu.VMEM((2, wide, most, 2 * share), BF16),
            pltpu.VMEM((wide, most, 2 * share), BF16),
            pltpu.VMEM((2, wide - 1, most, 2 * share), BF16),
            pltpu.VMEM((reach + 1, members, most, share), BF16),
            pltpu.VMEM((3, slots, width), BF16),
            pltpu.VMEM((2, 2, count, width), BF16),
            pltpu.VMEM((count, width), BF16),
            pltpu.VMEM((count, width), F32),
            pltpu.VMEM((groups, TABLE, count), F32),
            pltpu.VMEM((groups, TABLE, count), F32),
            pltpu.VMEM((2, most, 128), F32),
            pltpu.VMEM((2, most, 128), F32),
            pltpu.VMEM((count, count), BF16),
            pltpu.VMEM((count, count), BF16),
            pltpu.VMEM((2, members, 8, count), F32),
            dma((CHUNKS,)),
            dma((6,)),
            dma((2, steps, CHUNKS)),
            dma((2, steps, CHUNKS)),
            dma((2, steps)),
            dma((2, steps)),
            dma((2, steps, CHUNKS)),
            dma((2, steps, CHUNKS)),
            dma((2, experts, wide)),
            dma((2, experts, wide)),
            dma((2, experts, wide)),
            dma((2, experts, wide)),
            dma((2, experts, wide)),
            dma((2, experts, wide)),
            dma((2, experts, wide)),
            dma((2, experts, wide)),
            dma((2, members)),
            dma((2, members)),
            pltpu.SemaphoreType.REGULAR((2,)),
        ],
        compiler_params=pltpu.CompilerParams(
            collective_id=0, has_side_effects=True, vmem_limit_bytes=67043328
        ),
        name="layer",
    )(
        tokens,
        routes.T,
        route_weights.T,
        pre_gain[None, :],
        expert_gate,
        expert_up,
        expert_down,
        shared_gate,
        shared_up,
        shared_down,
        post_gain[None, :],
    )


def solution(mesh):
    in_specs = (
        P("ep", "tp"),
        P("ep", None),
        P("ep", None),
        P("tp"),
        P("ep", "tp", None),
        P("ep", "tp", None),
        P("ep", None, "tp"),
        P("tp", None),
        P("tp", None),
        P(None, "tp"),
        P("tp"),
    )
    return jax.shard_map(
        per_device, mesh=mesh, in_specs=in_specs, out_specs=P("ep", "tp"), check_vma=False
    )
```

```python
import functools

import jax
import jax.numpy as jnp
from jax import lax
from jax.experimental import pallas as pl
from jax.experimental.pallas import tpu as pltpu
from jax.sharding import PartitionSpec as P

epsilon = 1e-06
MESH = pl.DeviceIdType.MESH
F32, BF16 = jnp.float32, jnp.bfloat16
CHUNKS = 4
TABLE = 16
COLUMNS = 256


def ring_of(groups, width):
    if width < 2 or groups % width or groups // width < 2:
        return list(range(groups))
    depth = groups // width
    cycle = []
    for x in range(width):
        column = range(1, depth) if x % 2 == 0 else range(depth - 1, 0, -1)
        cycle += [z * width + x for z in column]
    return cycle + [x for x in range(width - 1, -1, -1)]


def dot(a, b):
    return jnp.dot(a, b, preferred_element_type=F32)


def dot_nt(a, b):
    return lax.dot_general(a, b, (((1,), (1,)), ((), ())), preferred_element_type=F32)


def iota(shape, axis):
    return lax.broadcasted_iota(jnp.int32, shape, axis).astype(F32)


def layer_kernel(
    cfg,
    tokens_hbm,
    routes_ref,
    weights_ref,
    gain_ref,
    gate_hbm,
    up_hbm,
    down_hbm,
    sgate_hbm,
    sup_hbm,
    sdown_hbm,
    mixed_hbm,
    scale_ref,
    tok,
    xbuf,
    mbuf,
    gate,
    up,
    down,
    sgate,
    sup,
    sdown,
    rows,
    hits,
    lifts,
    parts,
    got1,
    sums,
    got2,
    hid,
    made,
    back,
    farb,
    mix,
    slotv,
    wv,
    rinv,
    rwt,
    earlier,
    eye,
    squares,
    token_sem,
    load_sem,
    gs,
    gr,
    ms,
    mr,
    rs,
    s1s,
    s1r,
    s2s,
    s2r,
    s3s,
    s3r,
    s4s,
    s4r,
    ns,
    nr,
    credit,
):
    groups, members, experts, cap, fanout, ring, features = cfg
    count, width = mixed_hbm.shape
    reach = groups // 2
    wide = members // 2
    units = gate.shape[2]
    share = units // members
    chunk = count // CHUNKS
    slots = experts * cap
    far = 2 * reach - 1
    middle = count // 2
    packed = mbuf.shape[1]

    group, me = lax.axis_index("ep"), lax.axis_index("tp")
    core, row = lax.rem(me, 2), lax.div(me, 2)
    ahead, behind = jnp.int32(0), jnp.int32(0)
    for i, place in enumerate(ring):
        here = group == place
        ahead = jnp.where(here, ring[(i + 1) % groups], ahead)
        behind = jnp.where(here, ring[(i - 1) % groups], behind)
    gather_to = ({"ep": ahead}, {"ep": behind})
    return_to = ({"ep": behind}, {"ep": ahead})
    partner = {"tp": row * 2 + 1 - core}

    def peer_row(d):
        return lax.rem(row + d, wide)

    def remote(src, dst, send, recv, to):
        return pltpu.make_async_remote_copy(
            src_ref=src, dst_ref=dst, send_sem=send, recv_sem=recv, device_id=to, device_id_type=MESH
        )

    barrier = pltpu.get_barrier_semaphore()
    for to in gather_to:
        pl.semaphore_signal(barrier, inc=1, device_id=to, device_id_type=MESH)
    for d in range(1, members):
        pl.semaphore_signal(
            barrier, inc=1, device_id={"tp": lax.rem(me + d, members)}, device_id_type=MESH
        )

    def piece(c):
        at = c * chunk
        return pl.ds(at if isinstance(c, int) else pl.multiple_of(at, chunk), chunk)

    token_loads = [
        pltpu.make_async_copy(tokens_hbm.at[piece(c)], tok.at[piece(c)], token_sem.at[c])
        for c in range(CHUNKS)
    ]
    for load in token_loads:
        load.start()
    loads = [
        pltpu.make_async_copy(src, dst, load_sem.at[i])
        for i, (src, dst) in enumerate(
            (
                (gate_hbm, gate),
                (up_hbm, up),
                (sgate_hbm, sgate),
                (sup_hbm, sup),
                (down_hbm, down),
                (sdown_hbm, sdown),
            )
        )
    ]

    def gather(d, step, c, first=False, last=False):
        src = 0 if first or isinstance(step, int) and step == 1 else 2 * step - 3 + d
        dst = far if last else 2 * step - 1 + d
        return remote(
            xbuf.at[src, piece(c)],
            xbuf.at[dst, piece(c)],
            gs.at[d, 1 if last else 0],
            gr.at[d, step - 1, c],
            gather_to[d],
        )

    def gather_meta(d, step, first=False):
        src = 0 if first or isinstance(step, int) and step == 1 else 2 * step - 3 + d
        return remote(
            mbuf.at[src], mbuf.at[2 * step - 1 + d], ms.at[d], mr.at[d, step - 1], gather_to[d]
        )

    def sent(same, sem):
        remote(same, same, sem, sem, partner).wait_send()

    def half(d):
        return range(CHUNKS // 2) if d == 0 else range(CHUNKS // 2, CHUNKS)

    def scaled(c):
        xbuf[0, piece(c)] = (tok[piece(c)].astype(F32) * gain_ref[...]).astype(BF16)

    def diagonal(c):
        shape = (chunk, count)
        return iota(shape, 0) + float(c * chunk) == iota(shape, 1)

    def squares_of(c, value):
        column = jnp.sum(value * value, axis=1, keepdims=True)
        return jnp.sum(jnp.where(diagonal(c), column, 0.0), axis=0, keepdims=True)

    token_loads[0].wait()
    scaled(0)
    pl.semaphore_wait(barrier, 2 + members - 1)
    for d in range(2):
        gather(d, 1, 0, first=True).start()
    for c in range(1, CHUNKS):
        token_loads[c].wait()
    for load in loads:
        load.start()
    own_squares = jnp.zeros((1, count), F32)
    for c in range(CHUNKS):
        own_squares = own_squares + squares_of(c, tok[piece(c)].astype(F32))
    squares[0, me] = jnp.broadcast_to(own_squares, (8, count))

    def exchange_squares(which, meanwhile=lambda: None):
        copies = [
            remote(
                squares.at[which, me],
                squares.at[which, me],
                ns.at[d - 1],
                nr.at[d - 1],
                {"tp": lax.rem(me + d, members)},
            )
            for d in range(1, members)
        ]
        for copy in copies:
            copy.start()
        meanwhile()
        for copy in copies:
            copy.wait()
        total = squares[which, 0]
        for q in range(1, members):
            total = total + squares[which, q]
        return lax.rsqrt(total / features + epsilon)

    def finish_tokens():
        for c in range(1, CHUNKS):
            scaled(c)
        earlier[...] = jnp.where(iota(square, 0) < iota(square, 1), 1.0, 0.0).astype(BF16)
        eye[...] = jnp.where(iota(square, 0) == iota(square, 1), 1.0, 0.0).astype(BF16)

    square = (count, count)
    inverse_row = exchange_squares(0, finish_tokens)[0:1]
    high_weight = weights_ref[...].astype(BF16).astype(F32)
    high = inverse_row.astype(BF16).astype(F32)
    mid = (inverse_row - high).astype(BF16).astype(F32)
    mbuf[0] = jnp.concatenate(
        [
            routes_ref[...].astype(F32),
            high_weight,
            weights_ref[...] - high_weight,
            high,
            mid,
            inverse_row - high - mid,
        ]
        + [jnp.zeros((packed - 3 * fanout - 3, count), F32)],
        axis=0,
    ).astype(BF16)
    for d in range(2):
        gather_meta(d, 1, first=True).start()
        for c in range(1, CHUNKS):
            gather(d, 1, c, first=True).start()

    def poll(step, c):
        for d in range(2):
            if c == 0:
                gather_meta(d, step).wait_recv()

                @pl.when(step + 1 < reach + 1 - d)
                def _():
                    gather_meta(d, step + 1).start()

            gather(d, step, c).wait_recv()

            @pl.when(step + 1 < reach)
            def _():
                gather(d, step + 1, c).start()

            if c in half(d):

                @pl.when(step + 1 == reach)
                def _():
                    gather(d, reach, c, last=True).start()

    def tables(k):
        first = (group * experts).astype(F32)
        wanted = first + iota((TABLE, count), 0)
        present = jnp.zeros((TABLE, count), F32)
        weight = jnp.zeros((TABLE, count), F32)
        values = mbuf[k].astype(F32)
        for j in range(fanout):
            same = values[j : j + 1] == wanted
            present = present + jnp.where(same, 1.0, 0.0)
            exact = values[fanout + j : fanout + j + 1] + values[2 * fanout + j : 2 * fanout + j + 1]
            weight = weight + jnp.where(same, exact, 0.0)
        slot = dot(present.astype(BF16), earlier[...])
        slotv[k] = jnp.where(present > 0.0, slot, -1.0)
        wv[k] = weight
        at = 3 * fanout
        return values[at : at + 1] + values[at + 1 : at + 2] + values[at + 2 : at + 3]

    def row_values(turn, at, size, hit, inverse, weight):
        inv = jnp.sum(jnp.where(hit, inverse, 0.0), axis=1, keepdims=True)
        rinv[turn, at : at + size] = jnp.broadcast_to(inv, (size, 128))
        if weight is None:
            rwt[turn, at : at + size] = jnp.ones((size, 128), F32)
        else:
            value = jnp.sum(jnp.where(hit, weight, 0.0), axis=1, keepdims=True)
            rwt[turn, at : at + size] = jnp.broadcast_to(value, (size, 128))

    def prepare(turn, blocks, shared=False):
        n = len(blocks)
        for i, k in enumerate(blocks):
            inverse = tables(k)
            for e in range(experts):
                hit = iota((cap, count), 0) == slotv[k, e : e + 1]
                hits[i, e * cap : (e + 1) * cap] = jnp.where(hit, 1.0, 0.0).astype(BF16)
                row_values(turn, (e * n + i) * cap, cap, hit, inverse, wv[k, e : e + 1])
        if shared:
            for c in range(CHUNKS):
                row_values(turn, slots + c * chunk, chunk, diagonal(c), inverse, None)

    def put_parts(at, size, g, u):
        for q in range(members):
            parts[q // 2, q % 2, pl.ds(at, size), 0:share] = g[:, q * share : (q + 1) * share].astype(BF16)
            parts[q // 2, q % 2, pl.ds(at, size), share : 2 * share] = u[
                :, q * share : (q + 1) * share
            ].astype(BF16)

    def pick_rows(blocks, part=None):
        low, high = (0, count) if part is None else (part * middle, (part + 1) * middle)
        for i, k in enumerate(blocks):

            def pick(j, carry):
                at = pl.ds(pl.multiple_of(j * COLUMNS, COLUMNS), COLUMNS)
                picked = dot(hits[i, :, low:high], xbuf[k, low:high, at]).astype(BF16)
                for e in range(experts):
                    rows[e, i * cap : (i + 1) * cap, at] = picked[e * cap : (e + 1) * cap]
                return carry

            lax.fori_loop(0, width // COLUMNS, pick, 0)

    def pick_more(e, blocks):
        own = pl.ds(pl.multiple_of(e * cap, cap), cap)
        for i, k in enumerate(blocks):
            picked = dot(hits[i, own, middle:], xbuf[k, middle:]).astype(BF16)
            at = slice(i * cap, (i + 1) * cap)
            rows[e, at] = rows[e, at] + picked

    def project(e, n):
        taken = rows[e, 0 : n * cap]
        g, u = dot(taken, gate[e]), dot(taken, up[e])
        put_parts(pl.multiple_of(e * n * cap, n * cap), n * cap, g, u)

    def span(k, total):
        size = total // experts
        return pl.ds(k * size if isinstance(k, int) else pl.multiple_of(k * size, size), size)

    def core_copies(turn, k, total):
        return [
            remote(
                parts.at[:, 1 - core, span(k, total)],
                got1.at[turn, :, span(k, total)],
                s1s.at[k],
                s1r.at[turn, k],
                partner,
            )
        ]

    def row_copies(turn, k, total):
        return [
            remote(
                sums.at[peer_row(d), span(k, total)],
                got2.at[turn, d - 1, span(k, total)],
                s2s.at[k, d - 1],
                s2r.at[turn, k, d - 1],
                {"tp": peer_row(d) * 2 + core},
            )
            for d in range(1, wide)
        ]

    def hidden_row_copies(stage, k, total):
        turn = lax.rem(stage, 2)
        return [
            remote(
                hid.at[stage, row, core, span(k, total)],
                hid.at[stage, row, core, span(k, total)],
                s3s.at[turn, k, d - 1],
                s3r.at[turn, k, d - 1],
                {"tp": peer_row(d) * 2 + core},
            )
            for d in range(1, wide)
        ]

    def hidden_core_copies(stage, k, total):
        turn = lax.rem(stage, 2)
        return [
            remote(
                hid.at[stage, :, core, span(k, total)],
                hid.at[stage, :, core, span(k, total)],
                s4s.at[turn, k],
                s4r.at[turn, k],
                partner,
            )
        ]

    def start(copies):
        for copy in copies:
            copy.start()

    def wait(copies):
        for copy in copies:
            copy.wait()

    def add_core(turn, k, total):
        wait(core_copies(turn, k, total))
        at = span(k, total)
        for y in range(wide):
            mine = parts[y, core, at].astype(F32)
            sums[y, at] = (mine + got1[turn, y, at].astype(F32)).astype(BF16)
        start(row_copies(turn, k, total))

    def activate(stage, turn, k, total):
        wait(row_copies(turn, k, total))
        at = span(k, total)
        value = sums[row, at].astype(F32)
        for d in range(1, wide):
            value = value + got2[turn, d - 1, at].astype(F32)
        inv = rinv[turn, at, 0:share]
        g, u = value[:, 0:share] * inv, value[:, share : 2 * share] * inv
        hidden = g / (1.0 + jnp.exp(-g)) * u * rwt[turn, at, 0:share]
        hid[stage, row, core, at] = hidden.astype(BF16)
        start(hidden_row_copies(stage, k, total))

    def pass_hidden(stage, total):
        for k in range(experts):
            wait(hidden_row_copies(stage, k, total))
            start(hidden_core_copies(stage, k, total))

    def take_hidden(stage, total):
        for k in range(experts):
            wait(hidden_core_copies(stage, k, total))

    def send_parts(turn, n, total, more=None):
        def body(e, carry):
            if more is not None:
                pick_more(e, more)
            project(e, n)
            start(core_copies(turn, e, total))

            @pl.when(e > 0)
            def _():
                add_core(turn, e - 1, total)

            return carry

        lax.fori_loop(0, experts, body, 0)
        add_core(turn, experts - 1, total)

    def columns(at, k):
        slot_column = dot_nt(eye[...], slotv[k].astype(BF16))
        for e in range(experts):
            hit = iota((count, cap), 1) == slot_column[:, e : e + 1]
            lifts[at, :, e * cap : (e + 1) * cap] = jnp.where(hit, 1.0, 0.0).astype(BF16)

    def produce(stage, e, n, first):
        at = pl.ds(pl.multiple_of(e * n * cap, n * cap), n * cap)
        taken = jnp.concatenate([hid[stage, q // 2, q % 2, at] for q in range(members)], axis=1)
        result = dot(taken, down[e]).astype(BF16)
        for i in range(n):
            made[first + i, pl.ds(pl.multiple_of(e * cap, cap), cap)] = result[
                i * cap : (i + 1) * cap
            ]

    def produce_all(stage, n, first):
        def body(e, carry):
            produce(stage, e, n, first)
            return carry

        lax.fori_loop(0, experts, body, 0)

    def scatter(i, low, high, put):
        def tile(j, carry):
            at = pl.ds(pl.multiple_of(j * COLUMNS, COLUMNS), COLUMNS)
            put(at, dot(lifts[i, low:high], made[i, :, at]))
            return carry

        lax.fori_loop(0, width // COLUMNS, tile, 0)

    first_rows = slots + count
    pair_rows = 2 * slots

    prepare(0, [0], True)
    for i in range(4):
        loads[i].wait()
    pick_rows([0])

    def own_rows(e, carry):
        project(e, 1)
        return carry

    lax.fori_loop(0, experts, own_rows, 0)

    def shared_rows(c, carry):
        taken = xbuf[0, piece(c)]
        g, u = dot(taken, sgate[...]), dot(taken, sup[...])
        put_parts(pl.multiple_of(slots + c * chunk, 32), chunk, g, u)
        return carry

    lax.fori_loop(0, CHUNKS, shared_rows, 0)
    for k in range(experts):
        start(core_copies(0, k, first_rows))
    for k in range(experts):
        add_core(0, k, first_rows)
    poll(1, 0)
    prepare(1, [1, 2])
    for k in range(experts):
        activate(0, 0, k, first_rows)
        if k == 0:
            poll(1, 1)
            pick_rows([1, 2], 0)
        if k == experts - 2:
            poll(1, 2)
    poll(1, 3)

    def run_stage(s, carry):
        turn = lax.rem(s, 2)

        @pl.when(s == 2)
        def _():
            take_hidden(0, first_rows)

        @pl.when(s > 2)
        def _():
            take_hidden(s - 2, pair_rows)

        send_parts(turn, 2, pair_rows, [2 * s - 1, 2 * s])
        @pl.when(s == 1)
        def _():
            pass_hidden(0, first_rows)

        @pl.when(s > 1)
        def _():
            pass_hidden(s - 1, pair_rows)

        def more(c):
            @pl.when(s + 1 < reach)
            def _():
                poll(s + 1, c)

        more(0)

        @pl.when(s + 1 < reach)
        def _():
            prepare(1 - turn, [2 * s + 1, 2 * s + 2])

        @pl.when(s + 1 == reach)
        def _():
            gather_meta(0, reach).wait_recv()
            prepare(1 - turn, [far])
            columns(0, 2 * s - 1)
            columns(1, 2 * s)
            columns(2, far)

        for k in range(experts):
            activate(s, turn, k, pair_rows)
            if k == 0:
                more(1)

                @pl.when(s + 1 < reach)
                def _():
                    pick_rows([2 * s + 1, 2 * s + 2], 0)

            if k == experts - 2:
                more(2)
        more(3)
        return carry

    lax.fori_loop(1, reach, run_stage, 0)

    last, spare = reach - 1, reach % 2
    take_hidden(reach - 2, pair_rows if reach > 2 else first_rows)
    for d in range(2):
        for c in half(d):
            gather(d, reach, c, last=True).wait_recv()
    pick_rows([far])
    send_parts(spare, 1, slots)
    pass_hidden(last, pair_rows)
    loads[4].wait()
    for k in range(experts - 1):
        wait(hidden_core_copies(last, k, pair_rows))
        produce(last, k, 2, 0)

    for d in range(2):
        sent(xbuf.at[0 : reach - 1], gs.at[d, 0])
        sent(xbuf.at[0, 0:middle], gs.at[d, 1])
        sent(mbuf.at[0 : reach - d], ms.at[d])
    pl.semaphore_signal(credit.at[1], inc=1, device_id=return_to[0], device_id_type=MESH)
    pl.semaphore_signal(credit.at[0], inc=1, device_id=return_to[1], device_id_type=MESH)
    wait(hidden_core_copies(last, experts - 1, pair_rows))
    produce(last, experts - 1, 2, 0)

    def give(d, step, c, source, far_block=False):
        return remote(
            source.at[piece(c)],
            xbuf.at[2 * step - 1 + d, piece(c)],
            rs.at[d, 2 if far_block else lax.rem(step, 2)],
            gr.at[d, step - 1, c],
            return_to[d],
        )

    def into(side, i, low, high):
        def put(at, value):
            back[side, i, low:high, at] = value.astype(BF16)

        return put

    side = last % 2
    top = back.at[side]
    order = [list(half(1)) + list(half(0)), list(half(0)) + list(half(1))]
    for d in range(2):
        low = middle if d == 0 else 0
        scatter(d, low, low + middle, into(side, d, low, low + middle))
        pl.semaphore_wait(credit.at[d], 1)
        for j in range(CHUNKS // 2):
            give(d, 2, order[d][j], top.at[d]).start()

    for k in range(experts):
        activate(reach, spare, k, slots)
    for d in range(2):
        low = 0 if d == 0 else middle
        scatter(d, low, low + middle, into(side, d, low, low + middle))
    for k in range(experts):
        wait(hidden_row_copies(reach, k, slots))
        start(hidden_core_copies(reach, k, slots))
        if k > 0:
            wait(hidden_core_copies(reach, k - 1, slots))
            produce(reach, k - 1, 1, 2)
    wait(hidden_core_copies(reach, experts - 1, slots))
    produce(reach, experts - 1, 1, 2)

    def put_far(at, value):
        farb[:, at] = value.astype(BF16)

    scatter(2, 0, count, put_far)
    for j in range(CHUNKS // 2):
        for d in range(2):
            give(d, 1, order[d][CHUNKS // 2 + j], farb, True).start()

    def ready(s):
        produce_all(s, 2, 0)
        for i in range(2):
            columns(i, 2 * s - 1 + i)
            scatter(i, 0, count, into(lax.rem(s, 2), i, 0, count))

    if reach > 2:
        ready(reach - 2)

    def merge(d, step, c, source):
        give(d, step - 1, c, source).wait_recv()
        own = source[piece(c)].astype(F32)
        source[piece(c)] = (own + xbuf[2 * step - 3 + d, piece(c)].astype(F32)).astype(BF16)
        give(d, step, c, source).start()

    for j in range(CHUNKS // 2):
        for d in range(2):
            merge(d, 2, order[d][CHUNKS // 2 + j], top.at[d])

    for d in range(2):
        sent(farb.at[0:middle], rs.at[d, 2])

    def returning(step, carry):
        s = reach + 1 - step
        now = back.at[lax.rem(s, 2)]
        for j in range(CHUNKS):
            for d in range(2):
                merge(d, step, order[d][j], now.at[d])
        for d in range(2):
            sent(back.at[0, d], rs.at[d, lax.rem(step - 1, 2)])

        @pl.when(s > 1)
        def _():
            ready(s - 1)

        return carry

    lax.fori_loop(3, reach + 1, returning, 0)

    loads[5].wait()

    def put_own(at, value):
        taken = jnp.concatenate(
            [hid[0, q // 2, q % 2, slots : slots + count] for q in range(members)], axis=1
        )
        mix[:, at] = value + dot(taken, sdown[:, at])

    produce_all(0, 1, 0)
    columns(0, 0)
    scatter(0, 0, count, put_own)
    stores = [
        pltpu.make_async_copy(tok.at[piece(c)], mixed_hbm.at[piece(c)], token_sem.at[c])
        for c in range(CHUNKS)
    ]
    taken_chunks = [0] * CHUNKS
    total = jnp.zeros((1, count), F32)
    for j in range(CHUNKS):
        for d in range(2):
            c = order[d][j]
            give(d, reach, c, back.at[1, d]).wait_recv()
            value = mix[piece(c)] + xbuf[2 * reach - 1 + d, piece(c)].astype(F32)
            taken_chunks[c] += 1
            if taken_chunks[c] == 1:
                mix[piece(c)] = value
            else:
                tok[piece(c)] = value.astype(BF16)
                stores[c].start()
                total = total + squares_of(c, value)
    squares[1, me] = jnp.broadcast_to(total, (8, count))
    scale_ref[...] = exchange_squares(1)
    for c in range(CHUNKS):
        stores[c].wait()
    for d in range(2):
        sent(back.at[0, d], rs.at[d, reach % 2])


def finish_kernel(mixed_ref, scale_ref, post_ref, out_ref):
    shape = (mixed_ref.shape[0],) * 2
    same = iota(shape, 0) == iota(shape, 1)
    column = jnp.sum(jnp.where(same, scale_ref[0:1], 0.0), axis=1, keepdims=True)
    out_ref[...] = (mixed_ref[...].astype(F32) * column * post_ref[...]).astype(BF16)


def per_device(
    tokens,
    routes,
    route_weights,
    pre_gain,
    expert_gate,
    expert_up,
    expert_down,
    shared_gate,
    shared_up,
    shared_down,
    post_gain,
):
    members, groups = lax.axis_size("tp"), lax.axis_size("ep")
    count, width = tokens.shape
    fanout = routes.shape[1]
    experts, _, units = expert_gate.shape
    cap = 2 * count * fanout // (experts * groups)
    ring = tuple(ring_of(groups, members // 2))
    reach, wide = groups // 2, members // 2
    slots = experts * cap
    most = max(2 * slots, slots + count)
    share = units // members
    cfg = (groups, members, experts, cap, fanout, ring, float(width * members))

    vmem = pl.BlockSpec(memory_space=pltpu.VMEM)
    anywhere = pl.BlockSpec(memory_space=pl.ANY)
    dma = pltpu.SemaphoreType.DMA
    mixed, scale = pl.pallas_call(
        functools.partial(layer_kernel, cfg),
        out_shape=[
            jax.ShapeDtypeStruct((count, width), BF16),
            jax.ShapeDtypeStruct((8, count), F32),
        ],
        in_specs=[anywhere, vmem, vmem, vmem] + [anywhere] * 6,
        out_specs=[anywhere, vmem],
        scratch_shapes=[
            pltpu.VMEM((count, width), BF16),
            pltpu.VMEM((groups + 1, count, width), BF16),
            pltpu.VMEM((groups, -(-(3 * fanout + 3) // 16) * 16, count), BF16),
            pltpu.VMEM(expert_gate.shape, BF16),
            pltpu.VMEM(expert_up.shape, BF16),
            pltpu.VMEM(expert_down.shape, BF16),
            pltpu.VMEM(shared_gate.shape, BF16),
            pltpu.VMEM(shared_up.shape, BF16),
            pltpu.VMEM(shared_down.shape, BF16),
            pltpu.VMEM((experts, 2 * cap, width), BF16),
            pltpu.VMEM((2, slots, count), BF16),
            pltpu.VMEM((3, count, slots), BF16),
            pltpu.VMEM((wide, 2, most, 2 * share), BF16),
            pltpu.VMEM((2, wide, most, 2 * share), BF16),
            pltpu.VMEM((wide, most, 2 * share), BF16),
            pltpu.VMEM((2, wide - 1, most, 2 * share), BF16),
            pltpu.VMEM((reach + 1, wide, 2, most, share), BF16),
            pltpu.VMEM((3, slots, width), BF16),
            pltpu.VMEM((2, 2, count, width), BF16),
            pltpu.VMEM((count, width), BF16),
            pltpu.VMEM((count, width), F32),
            pltpu.VMEM((groups, TABLE, count), F32),
            pltpu.VMEM((groups, TABLE, count), F32),
            pltpu.VMEM((2, most, 128), F32),
            pltpu.VMEM((2, most, 128), F32),
            pltpu.VMEM((count, count), BF16),
            pltpu.VMEM((count, count), BF16),
            pltpu.VMEM((2, members, 8, count), F32),
            dma((CHUNKS,)),
            dma((6,)),
            dma((2, 2)),
            dma((2, reach, CHUNKS)),
            dma((2,)),
            dma((2, reach)),
            dma((2, 3)),
            dma((experts,)),
            dma((2, experts)),
            dma((experts, wide - 1)),
            dma((2, experts, wide - 1)),
            dma((2, experts, wide - 1)),
            dma((2, experts, wide - 1)),
            dma((2, experts)),
            dma((2, experts)),
            dma((members - 1,)),
            dma((members - 1,)),
            pltpu.SemaphoreType.REGULAR((2,)),
        ],
        compiler_params=pltpu.CompilerParams(
            collective_id=0, has_side_effects=True, vmem_limit_bytes=67043328
        ),
        name="layer",
    )(
        tokens,
        routes.T,
        route_weights.T,
        pre_gain[None, :],
        expert_gate,
        expert_up,
        expert_down,
        shared_gate,
        shared_up,
        shared_down,
    )
    block = count // 2
    return pl.pallas_call(
        finish_kernel,
        grid=(2,),
        in_specs=[
            pl.BlockSpec((block, width), lambda c: (c, 0)),
            pl.BlockSpec((8, block), lambda c: (0, c)),
            pl.BlockSpec((1, width), lambda c: (0, 0)),
        ],
        out_specs=pl.BlockSpec((block, width), lambda c: (c, 0)),
        out_shape=jax.ShapeDtypeStruct((count, width), BF16),
        name="finish",
    )(mixed, scale, post_gain[None, :])


def solution(mesh):
    in_specs = (
        P("ep", "tp"),
        P("ep", None),
        P("ep", None),
        P("tp"),
        P("ep", "tp", None),
        P("ep", "tp", None),
        P("ep", None, "tp"),
        P("tp", None),
        P("tp", None),
        P(None, "tp"),
        P("tp"),
    )
    return jax.shard_map(
        per_device, mesh=mesh, in_specs=in_specs, out_specs=P("ep", "tp"), check_vma=False
    )
```

```python
import functools

import jax
import jax.numpy as jnp
from jax import lax
from jax.experimental import pallas as pl
from jax.experimental.pallas import tpu as pltpu
from jax.sharding import PartitionSpec as P

epsilon = 1e-06
MESH = pl.DeviceIdType.MESH
F32, BF16 = jnp.float32, jnp.bfloat16
CHUNKS = 4
TABLE = 16
COLUMNS = 256


def ring_of(groups, width):
    if width < 2 or groups % width or groups // width < 2:
        return list(range(groups))
    depth = groups // width
    cycle = []
    for x in range(width):
        column = range(1, depth) if x % 2 == 0 else range(depth - 1, 0, -1)
        cycle += [z * width + x for z in column]
    return cycle + [x for x in range(width - 1, -1, -1)]


def dot(a, b):
    return jnp.dot(a, b, preferred_element_type=F32)


def dot_nt(a, b):
    return lax.dot_general(a, b, (((1,), (1,)), ((), ())), preferred_element_type=F32)


def iota(shape, axis):
    return lax.broadcasted_iota(jnp.int32, shape, axis).astype(F32)


def layer_kernel(
    cfg,
    tokens_hbm,
    routes_hbm,
    weights_hbm,
    gain_hbm,
    post_hbm,
    gate_hbm,
    up_hbm,
    down_hbm,
    sgate_hbm,
    sup_hbm,
    sdown_hbm,
    mixed_ref,
    scale_ref,
    routes_ref,
    weights_ref,
    gain_ref,
    post_ref,
    tok,
    xbuf,
    mbuf,
    gate,
    up,
    down,
    sgate,
    sup,
    sdown,
    rows,
    hits,
    lifts,
    parts,
    got1,
    sums,
    got2,
    hid,
    made,
    back,
    farb,
    mix,
    slotv,
    wv,
    rinv,
    rwt,
    earlier,
    eye,
    squares,
    small_sem,
    token_sem,
    load_sem,
    gs,
    gr,
    ms,
    mr,
    rs,
    s1s,
    s1r,
    s2s,
    s2r,
    s3s,
    s3r,
    s4s,
    s4r,
    ns,
    nr,
    credit,
):
    groups, members, experts, cap, fanout, ring, features = cfg
    count, width = mixed_ref.shape
    reach = groups // 2
    wide = members // 2
    units = gate.shape[2]
    share = units // members
    chunk = count // CHUNKS
    slots = experts * cap
    far = 2 * reach - 1
    middle = count // 2
    packed = mbuf.shape[1]

    group, me = lax.axis_index("ep"), lax.axis_index("tp")
    core, row = lax.rem(me, 2), lax.div(me, 2)
    ahead, behind = jnp.int32(0), jnp.int32(0)
    for i, place in enumerate(ring):
        here = group == place
        ahead = jnp.where(here, ring[(i + 1) % groups], ahead)
        behind = jnp.where(here, ring[(i - 1) % groups], behind)
    gather_to = ({"ep": ahead}, {"ep": behind})
    return_to = ({"ep": behind}, {"ep": ahead})
    partner = {"tp": row * 2 + 1 - core}

    def peer_row(d):
        return lax.rem(row + d, wide)

    def remote(src, dst, send, recv, to):
        return pltpu.make_async_remote_copy(
            src_ref=src, dst_ref=dst, send_sem=send, recv_sem=recv, device_id=to, device_id_type=MESH
        )

    def piece(c):
        at = c * chunk
        return pl.ds(at if isinstance(c, int) else pl.multiple_of(at, chunk), chunk)

    token_loads = [
        pltpu.make_async_copy(tokens_hbm.at[piece(c)], tok.at[piece(c)], token_sem.at[c])
        for c in range(CHUNKS)
    ]
    small_loads = [
        pltpu.make_async_copy(src, dst, small_sem.at[i])
        for i, (src, dst) in enumerate(
            (
                (gain_hbm, gain_ref),
                (routes_hbm, routes_ref),
                (weights_hbm, weights_ref),
                (post_hbm, post_ref),
            )
        )
    ]
    small_loads[0].start()
    for load in token_loads:
        load.start()
    barrier = pltpu.get_barrier_semaphore()
    for to in gather_to:
        pl.semaphore_signal(barrier, inc=1, device_id=to, device_id_type=MESH)
    for d in range(1, members):
        pl.semaphore_signal(
            barrier, inc=1, device_id={"tp": lax.rem(me + d, members)}, device_id_type=MESH
        )

    for load in small_loads[1:]:
        load.start()
    loads = [
        pltpu.make_async_copy(src, dst, load_sem.at[i])
        for i, (src, dst) in enumerate(
            (
                (gate_hbm, gate),
                (up_hbm, up),
                (sgate_hbm, sgate),
                (sup_hbm, sup),
                (down_hbm, down),
                (sdown_hbm, sdown),
            )
        )
    ]

    def gather(d, step, c, first=False, last=False):
        src = 0 if first or isinstance(step, int) and step == 1 else 2 * step - 3 + d
        dst = far if last else 2 * step - 1 + d
        return remote(
            xbuf.at[src, piece(c)],
            xbuf.at[dst, piece(c)],
            gs.at[d, 1 if last else 0],
            gr.at[d, step - 1, c],
            gather_to[d],
        )

    def gather_meta(d, step, first=False):
        src = 0 if first or isinstance(step, int) and step == 1 else 2 * step - 3 + d
        return remote(
            mbuf.at[src], mbuf.at[2 * step - 1 + d], ms.at[d], mr.at[d, step - 1], gather_to[d]
        )

    def sent(same, sem):
        remote(same, same, sem, sem, partner).wait_send()

    def half(d):
        return range(CHUNKS // 2) if d == 0 else range(CHUNKS // 2, CHUNKS)

    def scaled(c):
        xbuf[0, piece(c)] = (tok[piece(c)].astype(F32) * gain_ref[...]).astype(BF16)

    def diagonal(c):
        shape = (chunk, count)
        return iota(shape, 0) + float(c * chunk) == iota(shape, 1)

    def squares_of(c, value):
        column = jnp.sum(value * value, axis=1, keepdims=True)
        return jnp.sum(jnp.where(diagonal(c), column, 0.0), axis=0, keepdims=True)

    small_loads[0].wait()
    token_loads[0].wait()
    scaled(0)
    pl.semaphore_wait(barrier, 2 + members - 1)
    for d in range(2):
        gather(d, 1, 0, first=True).start()
    for c in range(1, CHUNKS):
        token_loads[c].wait()
    for load in loads:
        load.start()
    own_squares = jnp.zeros((1, count), F32)
    for c in range(CHUNKS):
        own_squares = own_squares + squares_of(c, tok[piece(c)].astype(F32))
    squares[0, me] = jnp.broadcast_to(own_squares, (8, count))

    def exchange_squares(which, meanwhile=lambda: None):
        copies = [
            remote(
                squares.at[which, me],
                squares.at[which, me],
                ns.at[d - 1],
                nr.at[d - 1],
                {"tp": lax.rem(me + d, members)},
            )
            for d in range(1, members)
        ]
        for copy in copies:
            copy.start()
        meanwhile()
        for copy in copies:
            copy.wait()
        total = squares[which, 0]
        for q in range(1, members):
            total = total + squares[which, q]
        return lax.rsqrt(total / features + epsilon)

    def finish_tokens():
        for c in range(1, CHUNKS):
            scaled(c)
        earlier[...] = jnp.where(iota(square, 0) < iota(square, 1), 1.0, 0.0).astype(BF16)
        eye[...] = jnp.where(iota(square, 0) == iota(square, 1), 1.0, 0.0).astype(BF16)

    square = (count, count)
    inverse_row = exchange_squares(0, finish_tokens)[0:1]
    for load in small_loads[1:]:
        load.wait()
    high_weight = weights_ref[...].astype(BF16).astype(F32)
    high = inverse_row.astype(BF16).astype(F32)
    mid = (inverse_row - high).astype(BF16).astype(F32)
    mbuf[0] = jnp.concatenate(
        [
            routes_ref[...].astype(F32),
            high_weight,
            weights_ref[...] - high_weight,
            high,
            mid,
            inverse_row - high - mid,
        ]
        + [jnp.zeros((packed - 3 * fanout - 3, count), F32)],
        axis=0,
    ).astype(BF16)
    for d in range(2):
        gather_meta(d, 1, first=True).start()
        for c in range(1, CHUNKS):
            gather(d, 1, c, first=True).start()

    def poll(step, c):
        for d in range(2):
            if c == 0:
                gather_meta(d, step).wait_recv()

                @pl.when(step + 1 < reach + 1 - d)
                def _():
                    gather_meta(d, step + 1).start()

            gather(d, step, c).wait_recv()

            @pl.when(step + 1 < reach)
            def _():
                gather(d, step + 1, c).start()

            if c in half(d):

                @pl.when(step + 1 == reach)
                def _():
                    gather(d, reach, c, last=True).start()

    def tables(k):
        first = (group * experts).astype(F32)
        wanted = first + iota((TABLE, count), 0)
        present = jnp.zeros((TABLE, count), F32)
        weight = jnp.zeros((TABLE, count), F32)
        values = mbuf[k].astype(F32)
        for j in range(fanout):
            same = values[j : j + 1] == wanted
            present = present + jnp.where(same, 1.0, 0.0)
            exact = values[fanout + j : fanout + j + 1] + values[2 * fanout + j : 2 * fanout + j + 1]
            weight = weight + jnp.where(same, exact, 0.0)
        slot = dot(present.astype(BF16), earlier[...])
        slotv[k] = jnp.where(present > 0.0, slot, -1.0)
        wv[k] = weight
        at = 3 * fanout
        return values[at : at + 1] + values[at + 1 : at + 2] + values[at + 2 : at + 3]

    def row_values(turn, at, size, hit, inverse, weight):
        inv = jnp.sum(jnp.where(hit, inverse, 0.0), axis=1, keepdims=True)
        rinv[turn, at : at + size] = jnp.broadcast_to(inv, (size, 128))
        if weight is None:
            rwt[turn, at : at + size] = jnp.ones((size, 128), F32)
        else:
            value = jnp.sum(jnp.where(hit, weight, 0.0), axis=1, keepdims=True)
            rwt[turn, at : at + size] = jnp.broadcast_to(value, (size, 128))

    def prepare(turn, blocks, shared=False):
        n = len(blocks)
        for i, k in enumerate(blocks):
            inverse = tables(k)
            for e in range(experts):
                hit = iota((cap, count), 0) == slotv[k, e : e + 1]
                hits[i, e * cap : (e + 1) * cap] = jnp.where(hit, 1.0, 0.0).astype(BF16)
                row_values(turn, (e * n + i) * cap, cap, hit, inverse, wv[k, e : e + 1])
        if shared:
            for c in range(CHUNKS):
                row_values(turn, slots + c * chunk, chunk, diagonal(c), inverse, None)

    def put_parts(at, size, g, u):
        for q in range(members):
            parts[q // 2, q % 2, pl.ds(at, size), 0:share] = g[:, q * share : (q + 1) * share].astype(BF16)
            parts[q // 2, q % 2, pl.ds(at, size), share : 2 * share] = u[
                :, q * share : (q + 1) * share
            ].astype(BF16)

    def pick_rows(blocks, part=None):
        low, high = (0, count) if part is None else (part * middle, (part + 1) * middle)
        for i, k in enumerate(blocks):

            def pick(j, carry):
                at = pl.ds(pl.multiple_of(j * COLUMNS, COLUMNS), COLUMNS)
                picked = dot(hits[i, :, low:high], xbuf[k, low:high, at]).astype(BF16)
                for e in range(experts):
                    rows[e, i * cap : (i + 1) * cap, at] = picked[e * cap : (e + 1) * cap]
                return carry

            lax.fori_loop(0, width // COLUMNS, pick, 0)

    def pick_more(e, blocks):
        own = pl.ds(pl.multiple_of(e * cap, cap), cap)
        for i, k in enumerate(blocks):
            picked = dot(hits[i, own, middle:], xbuf[k, middle:]).astype(BF16)
            at = slice(i * cap, (i + 1) * cap)
            rows[e, at] = rows[e, at] + picked

    def project(e, n):
        taken = rows[e, 0 : n * cap]
        g, u = dot(taken, gate[e]), dot(taken, up[e])
        put_parts(pl.multiple_of(e * n * cap, n * cap), n * cap, g, u)

    def span(k, total):
        size = total // experts
        return pl.ds(k * size if isinstance(k, int) else pl.multiple_of(k * size, size), size)

    def core_copies(turn, k, total):
        return [
            remote(
                parts.at[:, 1 - core, span(k, total)],
                got1.at[turn, :, span(k, total)],
                s1s.at[k],
                s1r.at[turn, k],
                partner,
            )
        ]

    def row_copies(turn, k, total):
        return [
            remote(
                sums.at[peer_row(d), span(k, total)],
                got2.at[turn, d - 1, span(k, total)],
                s2s.at[k, d - 1],
                s2r.at[turn, k, d - 1],
                {"tp": peer_row(d) * 2 + core},
            )
            for d in range(1, wide)
        ]

    def hidden_row_copies(stage, k, total):
        turn = lax.rem(stage, 2)
        return [
            remote(
                hid.at[stage, row, core, span(k, total)],
                hid.at[stage, row, core, span(k, total)],
                s3s.at[turn, k, d - 1],
                s3r.at[turn, k, d - 1],
                {"tp": peer_row(d) * 2 + core},
            )
            for d in range(1, wide)
        ]

    def hidden_core_copies(stage, k, total):
        turn = lax.rem(stage, 2)
        return [
            remote(
                hid.at[stage, :, core, span(k, total)],
                hid.at[stage, :, core, span(k, total)],
                s4s.at[turn, k],
                s4r.at[turn, k],
                partner,
            )
        ]

    def start(copies):
        for copy in copies:
            copy.start()

    def wait(copies):
        for copy in copies:
            copy.wait()

    def add_core(turn, k, total):
        wait(core_copies(turn, k, total))
        at = span(k, total)
        for y in range(wide):
            mine = parts[y, core, at].astype(F32)
            sums[y, at] = (mine + got1[turn, y, at].astype(F32)).astype(BF16)
        start(row_copies(turn, k, total))

    def activate(stage, turn, k, total):
        wait(row_copies(turn, k, total))
        at = span(k, total)
        value = sums[row, at].astype(F32)
        for d in range(1, wide):
            value = value + got2[turn, d - 1, at].astype(F32)
        inv = rinv[turn, at, 0:share]
        g, u = value[:, 0:share] * inv, value[:, share : 2 * share] * inv
        hidden = g / (1.0 + jnp.exp(-g)) * u * rwt[turn, at, 0:share]
        hid[stage, row, core, at] = hidden.astype(BF16)
        start(hidden_row_copies(stage, k, total))

    def pass_hidden(stage, total):
        for k in range(experts):
            wait(hidden_row_copies(stage, k, total))
            start(hidden_core_copies(stage, k, total))

    def take_hidden(stage, total):
        for k in range(experts):
            wait(hidden_core_copies(stage, k, total))

    def send_parts(turn, n, total, more=None):
        def body(e, carry):
            if more is not None:
                pick_more(e, more)
            project(e, n)
            start(core_copies(turn, e, total))

            @pl.when(e > 0)
            def _():
                add_core(turn, e - 1, total)

            return carry

        lax.fori_loop(0, experts, body, 0)
        add_core(turn, experts - 1, total)

    def columns(at, k):
        slot_column = dot_nt(eye[...], slotv[k].astype(BF16))
        for e in range(experts):
            hit = iota((count, cap), 1) == slot_column[:, e : e + 1]
            lifts[at, :, e * cap : (e + 1) * cap] = jnp.where(hit, 1.0, 0.0).astype(BF16)

    def produce(stage, e, n, first):
        at = pl.ds(pl.multiple_of(e * n * cap, n * cap), n * cap)
        taken = jnp.concatenate([hid[stage, q // 2, q % 2, at] for q in range(members)], axis=1)
        result = dot(taken, down[e]).astype(BF16)
        for i in range(n):
            made[first + i, pl.ds(pl.multiple_of(e * cap, cap), cap)] = result[
                i * cap : (i + 1) * cap
            ]

    def produce_all(stage, n, first):
        def body(e, carry):
            produce(stage, e, n, first)
            return carry

        lax.fori_loop(0, experts, body, 0)

    def scatter(i, low, high, put):
        def tile(j, carry):
            at = pl.ds(pl.multiple_of(j * COLUMNS, COLUMNS), COLUMNS)
            put(at, dot(lifts[i, low:high], made[i, :, at]))
            return carry

        lax.fori_loop(0, width // COLUMNS, tile, 0)

    first_rows = slots + count
    pair_rows = 2 * slots

    prepare(0, [0], True)
    for i in range(4):
        loads[i].wait()
    pick_rows([0])

    def own_rows(e, carry):
        project(e, 1)
        return carry

    lax.fori_loop(0, experts, own_rows, 0)

    def shared_rows(c, carry):
        taken = xbuf[0, piece(c)]
        g, u = dot(taken, sgate[...]), dot(taken, sup[...])
        put_parts(pl.multiple_of(slots + c * chunk, 32), chunk, g, u)
        return carry

    lax.fori_loop(0, CHUNKS, shared_rows, 0)
    for k in range(experts):
        start(core_copies(0, k, first_rows))
    for k in range(experts):
        add_core(0, k, first_rows)
    poll(1, 0)
    prepare(1, [1, 2])
    for k in range(experts):
        activate(0, 0, k, first_rows)
        if k == 0:
            poll(1, 1)
            pick_rows([1, 2], 0)
        if k == experts - 2:
            poll(1, 2)
    poll(1, 3)

    def run_stage(s, carry):
        turn = lax.rem(s, 2)

        @pl.when(s == 2)
        def _():
            take_hidden(0, first_rows)

        @pl.when(s > 2)
        def _():
            take_hidden(s - 2, pair_rows)

        send_parts(turn, 2, pair_rows, [2 * s - 1, 2 * s])
        @pl.when(s == 1)
        def _():
            pass_hidden(0, first_rows)

        @pl.when(s > 1)
        def _():
            pass_hidden(s - 1, pair_rows)

        def more(c):
            @pl.when(s + 1 < reach)
            def _():
                poll(s + 1, c)

        more(0)

        @pl.when(s + 1 < reach)
        def _():
            prepare(1 - turn, [2 * s + 1, 2 * s + 2])

        @pl.when(s + 1 == reach)
        def _():
            gather_meta(0, reach).wait_recv()
            prepare(1 - turn, [far])
            columns(0, 2 * s - 1)
            columns(1, 2 * s)
            columns(2, far)

        for k in range(experts):
            activate(s, turn, k, pair_rows)
            if k == 0:
                more(1)

                @pl.when(s + 1 < reach)
                def _():
                    pick_rows([2 * s + 1, 2 * s + 2], 0)

            if k == experts - 2:
                more(2)
        more(3)
        return carry

    lax.fori_loop(1, reach, run_stage, 0)

    last, spare = reach - 1, reach % 2
    take_hidden(reach - 2, pair_rows if reach > 2 else first_rows)
    for d in range(2):
        for c in half(d):
            gather(d, reach, c, last=True).wait_recv()
    pick_rows([far])
    send_parts(spare, 1, slots)
    pass_hidden(last, pair_rows)
    loads[4].wait()
    for k in range(experts - 1):
        wait(hidden_core_copies(last, k, pair_rows))
        produce(last, k, 2, 0)

    for d in range(2):
        sent(xbuf.at[0 : reach - 1], gs.at[d, 0])
        sent(xbuf.at[0, 0:middle], gs.at[d, 1])
        sent(mbuf.at[0 : reach - d], ms.at[d])
    pl.semaphore_signal(credit.at[1], inc=1, device_id=return_to[0], device_id_type=MESH)
    pl.semaphore_signal(credit.at[0], inc=1, device_id=return_to[1], device_id_type=MESH)
    wait(hidden_core_copies(last, experts - 1, pair_rows))
    produce(last, experts - 1, 2, 0)

    def give(d, step, c, source, far_block=False):
        return remote(
            source.at[piece(c)],
            xbuf.at[2 * step - 1 + d, piece(c)],
            rs.at[d, 2 if far_block else lax.rem(step, 2)],
            gr.at[d, step - 1, c],
            return_to[d],
        )

    def into(side, i, low, high):
        def put(at, value):
            back[side, i, low:high, at] = value.astype(BF16)

        return put

    side = last % 2
    top = back.at[side]
    order = [list(half(1)) + list(half(0)), list(half(0)) + list(half(1))]
    for j in range(CHUNKS // 2):
        for d in range(2):
            low = order[d][j] * chunk
            scatter(d, low, low + chunk, into(side, d, low, low + chunk))
            if j == 0:
                pl.semaphore_wait(credit.at[d], 1)
            give(d, 2, order[d][j], top.at[d]).start()

    for k in range(experts):
        activate(reach, spare, k, slots)
    for d in range(2):
        low = 0 if d == 0 else middle
        scatter(d, low, low + middle, into(side, d, low, low + middle))
    for k in range(experts):
        wait(hidden_row_copies(reach, k, slots))
        start(hidden_core_copies(reach, k, slots))
        if k > 0:
            wait(hidden_core_copies(reach, k - 1, slots))
            produce(reach, k - 1, 1, 2)
    wait(hidden_core_copies(reach, experts - 1, slots))
    produce(reach, experts - 1, 1, 2)

    def put_far(at, value):
        farb[:, at] = value.astype(BF16)

    scatter(2, 0, count, put_far)
    for j in range(CHUNKS // 2):
        for d in range(2):
            give(d, 1, order[d][CHUNKS // 2 + j], farb, True).start()

    def ready(s):
        produce_all(s, 2, 0)
        for i in range(2):
            columns(i, 2 * s - 1 + i)
            scatter(i, 0, count, into(lax.rem(s, 2), i, 0, count))

    if reach > 2:
        ready(reach - 2)

    def merge(d, step, c, source):
        give(d, step - 1, c, source).wait_recv()
        own = source[piece(c)].astype(F32)
        source[piece(c)] = (own + xbuf[2 * step - 3 + d, piece(c)].astype(F32)).astype(BF16)
        give(d, step, c, source).start()

    for j in range(CHUNKS // 2):
        for d in range(2):
            merge(d, 2, order[d][CHUNKS // 2 + j], top.at[d])

    for d in range(2):
        sent(farb.at[0:middle], rs.at[d, 2])

    def returning(step, carry):
        s = reach + 1 - step
        now = back.at[lax.rem(s, 2)]
        for j in range(CHUNKS):
            for d in range(2):
                merge(d, step, order[d][j], now.at[d])
        for d in range(2):
            sent(back.at[0, d], rs.at[d, lax.rem(step - 1, 2)])

        @pl.when(s > 1)
        def _():
            ready(s - 1)

        return carry

    lax.fori_loop(3, reach + 1, returning, 0)

    loads[5].wait()

    def put_own(at, value):
        taken = jnp.concatenate(
            [hid[0, q // 2, q % 2, slots : slots + count] for q in range(members)], axis=1
        )
        mix[:, at] = value + dot(taken, sdown[:, at])

    produce_all(0, 1, 0)
    columns(0, 0)
    scatter(0, 0, count, put_own)
    taken_chunks = [0] * CHUNKS
    total = jnp.zeros((1, count), F32)
    for j in range(CHUNKS):
        for d in range(2):
            c = order[d][j]
            give(d, reach, c, back.at[1, d]).wait_recv()
            value = mix[piece(c)] + xbuf[2 * reach - 1 + d, piece(c)].astype(F32)
            taken_chunks[c] += 1
            if taken_chunks[c] == 1:
                mix[piece(c)] = value
            else:
                mixed_ref[piece(c)] = (value * post_ref[...]).astype(BF16)
                total = total + squares_of(c, value)
    squares[1, me] = jnp.broadcast_to(total, (8, count))
    scale_ref[...] = exchange_squares(1)
    for d in range(2):
        sent(back.at[0, d], rs.at[d, reach % 2])


def finish_kernel(mixed_ref, scale_ref, out_ref):
    shape = (mixed_ref.shape[0],) * 2
    same = iota(shape, 0) == iota(shape, 1)
    column = jnp.sum(jnp.where(same, scale_ref[0:1], 0.0), axis=1, keepdims=True)
    out_ref[...] = (mixed_ref[...].astype(F32) * column).astype(BF16)


def per_device(
    tokens,
    routes,
    route_weights,
    pre_gain,
    expert_gate,
    expert_up,
    expert_down,
    shared_gate,
    shared_up,
    shared_down,
    post_gain,
):
    members, groups = lax.axis_size("tp"), lax.axis_size("ep")
    count, width = tokens.shape
    fanout = routes.shape[1]
    experts, _, units = expert_gate.shape
    cap = 2 * count * fanout // (experts * groups)
    ring = tuple(ring_of(groups, members // 2))
    reach, wide = groups // 2, members // 2
    slots = experts * cap
    most = max(2 * slots, slots + count)
    share = units // members
    cfg = (groups, members, experts, cap, fanout, ring, float(width * members))

    vmem = pl.BlockSpec(memory_space=pltpu.VMEM)
    anywhere = pl.BlockSpec(memory_space=pl.ANY)
    dma = pltpu.SemaphoreType.DMA
    mixed, scale = pl.pallas_call(
        functools.partial(layer_kernel, cfg),
        out_shape=[
            pltpu.VMEM((count, width), BF16),
            pltpu.VMEM((8, count), F32),
        ],
        in_specs=[anywhere] * 11,
        out_specs=[vmem, vmem],
        scratch_shapes=[
            pltpu.VMEM((fanout, count), routes.dtype),
            pltpu.VMEM((fanout, count), F32),
            pltpu.VMEM((1, width), F32),
            pltpu.VMEM((1, width), F32),
            pltpu.VMEM((count, width), BF16),
            pltpu.VMEM((groups + 1, count, width), BF16),
            pltpu.VMEM((groups, -(-(3 * fanout + 3) // 16) * 16, count), BF16),
            pltpu.VMEM(expert_gate.shape, BF16),
            pltpu.VMEM(expert_up.shape, BF16),
            pltpu.VMEM(expert_down.shape, BF16),
            pltpu.VMEM(shared_gate.shape, BF16),
            pltpu.VMEM(shared_up.shape, BF16),
            pltpu.VMEM(shared_down.shape, BF16),
            pltpu.VMEM((experts, 2 * cap, width), BF16),
            pltpu.VMEM((2, slots, count), BF16),
            pltpu.VMEM((3, count, slots), BF16),
            pltpu.VMEM((wide, 2, most, 2 * share), BF16),
            pltpu.VMEM((2, wide, most, 2 * share), BF16),
            pltpu.VMEM((wide, most, 2 * share), BF16),
            pltpu.VMEM((2, wide - 1, most, 2 * share), BF16),
            pltpu.VMEM((reach + 1, wide, 2, most, share), BF16),
            pltpu.VMEM((3, slots, width), BF16),
            pltpu.VMEM((2, 2, count, width), BF16),
            pltpu.VMEM((count, width), BF16),
            pltpu.VMEM((count, width), F32),
            pltpu.VMEM((groups, TABLE, count), F32),
            pltpu.VMEM((groups, TABLE, count), F32),
            pltpu.VMEM((2, most, 128), F32),
            pltpu.VMEM((2, most, 128), F32),
            pltpu.VMEM((count, count), BF16),
            pltpu.VMEM((count, count), BF16),
            pltpu.VMEM((2, members, 8, count), F32),
            dma((4,)),
            dma((CHUNKS,)),
            dma((6,)),
            dma((2, 2)),
            dma((2, reach, CHUNKS)),
            dma((2,)),
            dma((2, reach)),
            dma((2, 3)),
            dma((experts,)),
            dma((2, experts)),
            dma((experts, wide - 1)),
            dma((2, experts, wide - 1)),
            dma((2, experts, wide - 1)),
            dma((2, experts, wide - 1)),
            dma((2, experts)),
            dma((2, experts)),
            dma((members - 1,)),
            dma((members - 1,)),
            pltpu.SemaphoreType.REGULAR((2,)),
        ],
        compiler_params=pltpu.CompilerParams(
            collective_id=0, has_side_effects=True, vmem_limit_bytes=66977792 - 2 * count * width - 32 * count
        ),
        name="layer",
    )(
        tokens,
        routes.T,
        route_weights.T,
        pre_gain[None, :],
        post_gain[None, :],
        expert_gate,
        expert_up,
        expert_down,
        shared_gate,
        shared_up,
        shared_down,
    )
    mixed = pltpu.with_memory_space_constraint(mixed, pltpu.VMEM)
    scale = pltpu.with_memory_space_constraint(scale, pltpu.VMEM)
    block = count // 2
    return pl.pallas_call(
        finish_kernel,
        grid=(2,),
        in_specs=[
            pl.BlockSpec((block, width), lambda c: (c, 0)),
            pl.BlockSpec((8, block), lambda c: (0, c)),
        ],
        out_specs=pl.BlockSpec((block, width), lambda c: (c, 0)),
        out_shape=jax.ShapeDtypeStruct((count, width), BF16),
        name="finish",
    )(mixed, scale)


def solution(mesh):
    in_specs = (
        P("ep", "tp"),
        P("ep", None),
        P("ep", None),
        P("tp"),
        P("ep", "tp", None),
        P("ep", "tp", None),
        P("ep", None, "tp"),
        P("tp", None),
        P("tp", None),
        P(None, "tp"),
        P("tp"),
    )
    return jax.shard_map(
        per_device, mesh=mesh, in_specs=in_specs, out_specs=P("ep", "tp"), check_vma=False
    )
```

```python
import functools

import jax
import jax.numpy as jnp
from jax import lax
from jax.experimental import pallas as pl
from jax.experimental.pallas import tpu as pltpu
from jax.sharding import PartitionSpec as P

epsilon = 1e-06
MESH = pl.DeviceIdType.MESH
F32, BF16 = jnp.float32, jnp.bfloat16
CHUNKS = 4
TABLE = 16
COLUMNS = 256


def ring_of(groups, width):
    if width < 2 or groups % width or groups // width < 2:
        return list(range(groups))
    depth = groups // width
    cycle = []
    for x in range(width):
        column = range(1, depth) if x % 2 == 0 else range(depth - 1, 0, -1)
        cycle += [z * width + x for z in column]
    return cycle + [x for x in range(width - 1, -1, -1)]


def dot(a, b):
    return jnp.dot(a, b, preferred_element_type=F32)


def dot_nt(a, b):
    return lax.dot_general(a, b, (((1,), (1,)), ((), ())), preferred_element_type=F32)


def iota(shape, axis):
    return lax.broadcasted_iota(jnp.int32, shape, axis).astype(F32)


def layer_kernel(
    cfg,
    tokens_hbm,
    routes_hbm,
    weights_hbm,
    gain_hbm,
    post_hbm,
    gate_hbm,
    up_hbm,
    down_hbm,
    sgate_hbm,
    sup_hbm,
    sdown_hbm,
    mixed_ref,
    scale_ref,
    routes_ref,
    weights_ref,
    gain_ref,
    post_ref,
    tok,
    xbuf,
    mbuf,
    gate,
    up,
    down,
    sgate,
    sup,
    sdown,
    rows,
    hits,
    lifts,
    parts,
    got1,
    sums,
    got2,
    hid,
    made,
    back,
    farb,
    mix,
    slotv,
    wv,
    rinv,
    rwt,
    earlier,
    eye,
    squares,
    small_sem,
    token_sem,
    load_sem,
    gs,
    gr,
    ms,
    mr,
    rs,
    s1s,
    s1r,
    s2s,
    s2r,
    s3s,
    s3r,
    s4s,
    s4r,
    ns,
    nr,
    credit,
):
    groups, members, experts, cap, fanout, ring, features = cfg
    count, width = mixed_ref.shape
    reach = groups // 2
    wide = members // 2
    units = gate.shape[2]
    share = units // members
    chunk = count // CHUNKS
    slots = experts * cap
    far = 2 * reach - 1
    middle = count // 2
    packed = mbuf.shape[1]

    group, me = lax.axis_index("ep"), lax.axis_index("tp")
    core, row = lax.rem(me, 2), lax.div(me, 2)
    ahead, behind = jnp.int32(0), jnp.int32(0)
    for i, place in enumerate(ring):
        here = group == place
        ahead = jnp.where(here, ring[(i + 1) % groups], ahead)
        behind = jnp.where(here, ring[(i - 1) % groups], behind)
    gather_to = ({"ep": ahead}, {"ep": behind})
    return_to = ({"ep": behind}, {"ep": ahead})
    partner = {"tp": row * 2 + 1 - core}

    def peer_row(d):
        return lax.rem(row + d, wide)

    def remote(src, dst, send, recv, to):
        return pltpu.make_async_remote_copy(
            src_ref=src, dst_ref=dst, send_sem=send, recv_sem=recv, device_id=to, device_id_type=MESH
        )

    def piece(c):
        at = c * chunk
        return pl.ds(at if isinstance(c, int) else pl.multiple_of(at, chunk), chunk)

    token_loads = [
        pltpu.make_async_copy(tokens_hbm.at[piece(c)], tok.at[piece(c)], token_sem.at[c])
        for c in range(CHUNKS)
    ]
    small_loads = [
        pltpu.make_async_copy(src, dst, small_sem.at[i])
        for i, (src, dst) in enumerate(
            (
                (gain_hbm, gain_ref),
                (routes_hbm, routes_ref),
                (weights_hbm, weights_ref),
                (post_hbm, post_ref),
            )
        )
    ]
    small_loads[0].start()
    for load in token_loads:
        load.start()
    barrier = pltpu.get_barrier_semaphore()
    for to in gather_to:
        pl.semaphore_signal(barrier, inc=1, device_id=to, device_id_type=MESH)
    for d in range(1, members):
        pl.semaphore_signal(
            barrier, inc=1, device_id={"tp": lax.rem(me + d, members)}, device_id_type=MESH
        )

    for load in small_loads[1:]:
        load.start()
    loads = [
        pltpu.make_async_copy(src, dst, load_sem.at[i])
        for i, (src, dst) in enumerate(
            (
                (gate_hbm, gate),
                (up_hbm, up),
                (sgate_hbm, sgate),
                (sup_hbm, sup),
                (down_hbm, down),
                (sdown_hbm, sdown),
            )
        )
    ]

    def gather(d, step, c, first=False, last=False):
        src = 0 if first or isinstance(step, int) and step == 1 else 2 * step - 3 + d
        dst = far if last else 2 * step - 1 + d
        return remote(
            xbuf.at[src, piece(c)],
            xbuf.at[dst, piece(c)],
            gs.at[d, 1 if last else 0],
            gr.at[d, step - 1, c],
            gather_to[d],
        )

    def gather_meta(d, step, first=False):
        src = 0 if first or isinstance(step, int) and step == 1 else 2 * step - 3 + d
        return remote(
            mbuf.at[src], mbuf.at[2 * step - 1 + d], ms.at[d], mr.at[d, step - 1], gather_to[d]
        )

    def sent(same, sem):
        remote(same, same, sem, sem, partner).wait_send()

    def half(d):
        return range(CHUNKS // 2) if d == 0 else range(CHUNKS // 2, CHUNKS)

    def scaled(c):
        xbuf[0, piece(c)] = (tok[piece(c)].astype(F32) * gain_ref[...]).astype(BF16)

    def diagonal(c):
        shape = (chunk, count)
        return iota(shape, 0) + float(c * chunk) == iota(shape, 1)

    def squares_of(c, value):
        column = jnp.sum(value * value, axis=1, keepdims=True)
        return jnp.sum(jnp.where(diagonal(c), column, 0.0), axis=0, keepdims=True)

    small_loads[0].wait()
    token_loads[0].wait()
    scaled(0)
    pl.semaphore_wait(barrier, 2 + members - 1)
    for d in range(2):
        gather(d, 1, 0, first=True).start()
    for c in range(1, CHUNKS):
        token_loads[c].wait()
    for load in loads:
        load.start()
    own_squares = jnp.zeros((1, count), F32)
    for c in range(CHUNKS):
        own_squares = own_squares + squares_of(c, tok[piece(c)].astype(F32))
    squares[0, me] = own_squares

    def exchange_squares(which, meanwhile=lambda: None):
        copies = [
            remote(
                squares.at[which, me],
                squares.at[which, me],
                ns.at[d - 1],
                nr.at[d - 1],
                {"tp": lax.rem(me + d, members)},
            )
            for d in range(1, members)
        ]
        for copy in copies:
            copy.start()
        meanwhile()
        for copy in copies:
            copy.wait()
        total = squares[which, 0]
        for q in range(1, members):
            total = total + squares[which, q]
        return lax.rsqrt(total / features + epsilon)

    def finish_tokens():
        for c in range(1, CHUNKS):
            scaled(c)
        earlier[...] = jnp.where(iota(square, 0) < iota(square, 1), 1.0, 0.0).astype(BF16)
        eye[...] = jnp.where(iota(square, 0) == iota(square, 1), 1.0, 0.0).astype(BF16)

    square = (count, count)
    inverse_row = exchange_squares(0, finish_tokens)
    for load in small_loads[1:]:
        load.wait()
    high_weight = weights_ref[...].astype(BF16).astype(F32)
    high = inverse_row.astype(BF16).astype(F32)
    mid = (inverse_row - high).astype(BF16).astype(F32)
    mbuf[0] = jnp.concatenate(
        [
            routes_ref[...].astype(F32),
            high_weight,
            weights_ref[...] - high_weight,
            high,
            mid,
            inverse_row - high - mid,
        ]
        + [jnp.zeros((packed - 3 * fanout - 3, count), F32)],
        axis=0,
    ).astype(BF16)
    for d in range(2):
        gather_meta(d, 1, first=True).start()
        for c in range(1, CHUNKS):
            gather(d, 1, c, first=True).start()

    def poll(step, c):
        for d in range(2):
            if c == 0:
                gather_meta(d, step).wait_recv()

                @pl.when(step + 1 < reach + 1 - d)
                def _():
                    gather_meta(d, step + 1).start()

            gather(d, step, c).wait_recv()

            @pl.when(step + 1 < reach)
            def _():
                gather(d, step + 1, c).start()

            if c in half(d):

                @pl.when(step + 1 == reach)
                def _():
                    gather(d, reach, c, last=True).start()

    def tables(k):
        first = (group * experts).astype(F32)
        wanted = first + iota((TABLE, count), 0)
        present = jnp.zeros((TABLE, count), F32)
        weight = jnp.zeros((TABLE, count), F32)
        values = mbuf[k].astype(F32)
        for j in range(fanout):
            same = values[j : j + 1] == wanted
            present = present + jnp.where(same, 1.0, 0.0)
            exact = values[fanout + j : fanout + j + 1] + values[2 * fanout + j : 2 * fanout + j + 1]
            weight = weight + jnp.where(same, exact, 0.0)
        slot = dot(present.astype(BF16), earlier[...])
        slotv[k] = jnp.where(present > 0.0, slot, -1.0)
        wv[k] = weight
        at = 3 * fanout
        return values[at : at + 1] + values[at + 1 : at + 2] + values[at + 2 : at + 3]

    def row_values(turn, at, size, hit, inverse, weight):
        inv = jnp.sum(jnp.where(hit, inverse, 0.0), axis=1, keepdims=True)
        rinv[turn, at : at + size] = jnp.broadcast_to(inv, (size, 128))
        if weight is None:
            rwt[turn, at : at + size] = jnp.ones((size, 128), F32)
        else:
            value = jnp.sum(jnp.where(hit, weight, 0.0), axis=1, keepdims=True)
            rwt[turn, at : at + size] = jnp.broadcast_to(value, (size, 128))

    def prepare(turn, blocks, shared=False):
        n = len(blocks)
        for i, k in enumerate(blocks):
            inverse = tables(k)
            for e in range(experts):
                hit = iota((cap, count), 0) == slotv[k, e : e + 1]
                hits[i, e * cap : (e + 1) * cap] = jnp.where(hit, 1.0, 0.0).astype(BF16)
                row_values(turn, (e * n + i) * cap, cap, hit, inverse, wv[k, e : e + 1])
        if shared:
            for c in range(CHUNKS):
                row_values(turn, slots + c * chunk, chunk, diagonal(c), inverse, None)

    def put_parts(at, size, g, u):
        for q in range(members):
            parts[q // 2, q % 2, pl.ds(at, size), 0:share] = g[:, q * share : (q + 1) * share].astype(BF16)
            parts[q // 2, q % 2, pl.ds(at, size), share : 2 * share] = u[
                :, q * share : (q + 1) * share
            ].astype(BF16)

    def pick_rows(blocks, part=None):
        low, high = (0, count) if part is None else (part * middle, (part + 1) * middle)
        for i, k in enumerate(blocks):

            def pick(j, carry):
                at = pl.ds(pl.multiple_of(j * COLUMNS, COLUMNS), COLUMNS)
                picked = dot(hits[i, :, low:high], xbuf[k, low:high, at]).astype(BF16)
                for e in range(experts):
                    rows[e, i * cap : (i + 1) * cap, at] = picked[e * cap : (e + 1) * cap]
                return carry

            lax.fori_loop(0, width // COLUMNS, pick, 0)

    def pick_more(e, blocks):
        own = pl.ds(pl.multiple_of(e * cap, cap), cap)
        for i, k in enumerate(blocks):
            picked = dot(hits[i, own, middle:], xbuf[k, middle:]).astype(BF16)
            at = slice(i * cap, (i + 1) * cap)
            rows[e, at] = rows[e, at] + picked

    def project(e, n):
        taken = rows[e, 0 : n * cap]
        g, u = dot(taken, gate[e]), dot(taken, up[e])
        put_parts(pl.multiple_of(e * n * cap, n * cap), n * cap, g, u)

    def span(k, total):
        size = total // experts
        return pl.ds(k * size if isinstance(k, int) else pl.multiple_of(k * size, size), size)

    def core_copies(turn, k, total):
        return [
            remote(
                parts.at[:, 1 - core, span(k, total)],
                got1.at[turn, :, span(k, total)],
                s1s.at[k],
                s1r.at[turn, k],
                partner,
            )
        ]

    def row_copies(turn, k, total):
        return [
            remote(
                sums.at[peer_row(d), span(k, total)],
                got2.at[turn, d - 1, span(k, total)],
                s2s.at[k, d - 1],
                s2r.at[turn, k, d - 1],
                {"tp": peer_row(d) * 2 + core},
            )
            for d in range(1, wide)
        ]

    def hidden_row_copies(stage, k, total):
        turn = lax.rem(stage, 2)
        return [
            remote(
                hid.at[stage, row, core, span(k, total)],
                hid.at[stage, row, core, span(k, total)],
                s3s.at[turn, k, d - 1],
                s3r.at[turn, k, d - 1],
                {"tp": peer_row(d) * 2 + core},
            )
            for d in range(1, wide)
        ]

    def hidden_core_copies(stage, k, total):
        turn = lax.rem(stage, 2)
        return [
            remote(
                hid.at[stage, :, core, span(k, total)],
                hid.at[stage, :, core, span(k, total)],
                s4s.at[turn, k],
                s4r.at[turn, k],
                partner,
            )
        ]

    def start(copies):
        for copy in copies:
            copy.start()

    def wait(copies):
        for copy in copies:
            copy.wait()

    def add_core(turn, k, total):
        wait(core_copies(turn, k, total))
        at = span(k, total)
        for y in range(wide):
            mine = parts[y, core, at].astype(F32)
            sums[y, at] = (mine + got1[turn, y, at].astype(F32)).astype(BF16)
        start(row_copies(turn, k, total))

    def activate(stage, turn, k, total):
        wait(row_copies(turn, k, total))
        at = span(k, total)
        value = sums[row, at].astype(F32)
        for d in range(1, wide):
            value = value + got2[turn, d - 1, at].astype(F32)
        inv = rinv[turn, at, 0:share]
        g, u = value[:, 0:share] * inv, value[:, share : 2 * share] * inv
        hidden = g / (1.0 + jnp.exp(-g)) * u * rwt[turn, at, 0:share]
        hid[stage, row, core, at] = hidden.astype(BF16)
        start(hidden_row_copies(stage, k, total))

    def pass_one(stage, k, total):
        wait(hidden_row_copies(stage, k, total))
        start(hidden_core_copies(stage, k, total))

    def pass_hidden(stage, total):
        for k in range(experts):
            pass_one(stage, k, total)

    def take_hidden(stage, total):
        for k in range(experts):
            wait(hidden_core_copies(stage, k, total))

    def send_parts(turn, n, total, more=None, beside=None):
        def body(e, carry):
            if more is not None:
                pick_more(e, more)
            project(e, n)
            start(core_copies(turn, e, total))

            @pl.when(e > 0)
            def _():
                add_core(turn, e - 1, total)
                if beside is not None:
                    beside(e - 1)

            return carry

        lax.fori_loop(0, experts, body, 0)
        add_core(turn, experts - 1, total)

    def columns(at, k):
        slot_column = dot_nt(eye[...], slotv[k].astype(BF16))
        for e in range(experts):
            hit = iota((count, cap), 1) == slot_column[:, e : e + 1]
            lifts[at, :, e * cap : (e + 1) * cap] = jnp.where(hit, 1.0, 0.0).astype(BF16)

    def produce(stage, e, n, first):
        at = pl.ds(pl.multiple_of(e * n * cap, n * cap), n * cap)
        taken = jnp.concatenate([hid[stage, q // 2, q % 2, at] for q in range(members)], axis=1)
        result = dot(taken, down[e]).astype(BF16)
        for i in range(n):
            made[first + i, pl.ds(pl.multiple_of(e * cap, cap), cap)] = result[
                i * cap : (i + 1) * cap
            ]

    def produce_all(stage, n, first):
        def body(e, carry):
            produce(stage, e, n, first)
            return carry

        lax.fori_loop(0, experts, body, 0)

    def scatter(i, low, high, put):
        def tile(j, carry):
            at = pl.ds(pl.multiple_of(j * COLUMNS, COLUMNS), COLUMNS)
            put(at, dot(lifts[i, low:high], made[i, :, at]))
            return carry

        lax.fori_loop(0, width // COLUMNS, tile, 0)

    first_rows = slots + count
    pair_rows = 2 * slots

    prepare(0, [0], True)
    for i in range(4):
        loads[i].wait()
    pick_rows([0])

    def own_rows(e, carry):
        project(e, 1)
        return carry

    lax.fori_loop(0, experts, own_rows, 0)

    def shared_rows(c, carry):
        taken = xbuf[0, piece(c)]
        g, u = dot(taken, sgate[...]), dot(taken, sup[...])
        put_parts(pl.multiple_of(slots + c * chunk, 32), chunk, g, u)
        return carry

    lax.fori_loop(0, CHUNKS, shared_rows, 0)
    for k in range(experts):
        start(core_copies(0, k, first_rows))
    for k in range(experts):
        add_core(0, k, first_rows)
    poll(1, 0)
    prepare(1, [1, 2])
    for k in range(experts):
        activate(0, 0, k, first_rows)
        if k == 0:
            poll(1, 1)
            pick_rows([1, 2], 0)
        if k == experts - 2:
            poll(1, 2)
    poll(1, 3)

    def run_stage(s, carry):
        turn = lax.rem(s, 2)

        @pl.when(s == 2)
        def _():
            take_hidden(0, first_rows)

        @pl.when(s > 2)
        def _():
            take_hidden(s - 2, pair_rows)

        send_parts(turn, 2, pair_rows, [2 * s - 1, 2 * s])
        @pl.when(s == 1)
        def _():
            pass_hidden(0, first_rows)

        @pl.when(s > 1)
        def _():
            pass_hidden(s - 1, pair_rows)

        def more(c):
            @pl.when(s + 1 < reach)
            def _():
                poll(s + 1, c)

        more(0)

        @pl.when(s + 1 < reach)
        def _():
            prepare(1 - turn, [2 * s + 1, 2 * s + 2])

        @pl.when(s + 1 == reach)
        def _():
            gather_meta(0, reach).wait_recv()
            prepare(1 - turn, [far])
            columns(0, 2 * s - 1)
            columns(1, 2 * s)
            columns(2, far)

        for k in range(experts):
            activate(s, turn, k, pair_rows)
            if k == 0:
                more(1)

                @pl.when(s + 1 < reach)
                def _():
                    pick_rows([2 * s + 1, 2 * s + 2], 0)

            if k == experts - 2:
                more(2)
        more(3)
        return carry

    lax.fori_loop(1, reach, run_stage, 0)

    last, spare = reach - 1, reach % 2
    take_hidden(reach - 2, pair_rows if reach > 2 else first_rows)
    for d in range(2):
        for c in half(d):
            gather(d, reach, c, last=True).wait_recv()
    pick_rows([far])
    send_parts(spare, 1, slots, beside=lambda k: pass_one(last, k, pair_rows))
    pass_one(last, experts - 1, pair_rows)
    loads[4].wait()
    for k in range(experts - 1):
        wait(hidden_core_copies(last, k, pair_rows))
        produce(last, k, 2, 0)

    for d in range(2):
        sent(xbuf.at[0 : reach - 1], gs.at[d, 0])
        sent(xbuf.at[0, 0:middle], gs.at[d, 1])
        sent(mbuf.at[0 : reach - d], ms.at[d])
    pl.semaphore_signal(credit.at[1], inc=1, device_id=return_to[0], device_id_type=MESH)
    pl.semaphore_signal(credit.at[0], inc=1, device_id=return_to[1], device_id_type=MESH)
    wait(hidden_core_copies(last, experts - 1, pair_rows))
    produce(last, experts - 1, 2, 0)

    def give(d, step, c, source, far_block=False):
        return remote(
            source.at[piece(c)],
            xbuf.at[2 * step - 1 + d, piece(c)],
            rs.at[d, 2 if far_block else lax.rem(step, 2)],
            gr.at[d, step - 1, c],
            return_to[d],
        )

    def into(side, i, low, high):
        def put(at, value):
            back[side, i, low:high, at] = value.astype(BF16)

        return put

    side = last % 2
    top = back.at[side]
    order = [list(half(1)) + list(half(0)), list(half(0)) + list(half(1))]
    for j in range(CHUNKS // 2):
        for d in range(2):
            low = order[d][j] * chunk
            scatter(d, low, low + chunk, into(side, d, low, low + chunk))
            if j == 0:
                pl.semaphore_wait(credit.at[d], 1)
            give(d, 2, order[d][j], top.at[d]).start()

    for k in range(experts):
        activate(reach, spare, k, slots)
    for d in range(2):
        low = 0 if d == 0 else middle
        scatter(d, low, low + middle, into(side, d, low, low + middle))
    for k in range(experts):
        wait(hidden_row_copies(reach, k, slots))
        start(hidden_core_copies(reach, k, slots))
        if k > 0:
            wait(hidden_core_copies(reach, k - 1, slots))
            produce(reach, k - 1, 1, 2)
    wait(hidden_core_copies(reach, experts - 1, slots))
    produce(reach, experts - 1, 1, 2)

    def put_far(at, value):
        farb[:, at] = value.astype(BF16)

    scatter(2, 0, count, put_far)
    for j in range(CHUNKS // 2):
        for d in range(2):
            give(d, 1, order[d][CHUNKS // 2 + j], farb, True).start()

    def ready(s):
        produce_all(s, 2, 0)
        for i in range(2):
            columns(i, 2 * s - 1 + i)
            scatter(i, 0, count, into(lax.rem(s, 2), i, 0, count))

    if reach > 2:
        ready(reach - 2)

    def merge(d, step, c, source):
        give(d, step - 1, c, source).wait_recv()
        own = source[piece(c)].astype(F32)
        source[piece(c)] = (own + xbuf[2 * step - 3 + d, piece(c)].astype(F32)).astype(BF16)
        give(d, step, c, source).start()

    for j in range(CHUNKS // 2):
        for d in range(2):
            merge(d, 2, order[d][CHUNKS // 2 + j], top.at[d])

    for d in range(2):
        sent(farb.at[0:middle], rs.at[d, 2])

    def returning(step, carry):
        s = reach + 1 - step
        now = back.at[lax.rem(s, 2)]
        for j in range(CHUNKS):
            for d in range(2):
                merge(d, step, order[d][j], now.at[d])
        for d in range(2):
            sent(back.at[0, d], rs.at[d, lax.rem(step - 1, 2)])

        @pl.when(s > 1)
        def _():
            ready(s - 1)

        return carry

    lax.fori_loop(3, reach + 1, returning, 0)

    loads[5].wait()

    def put_own(at, value):
        taken = jnp.concatenate(
            [hid[0, q // 2, q % 2, slots : slots + count] for q in range(members)], axis=1
        )
        mix[:, at] = value + dot(taken, sdown[:, at])

    produce_all(0, 1, 0)
    columns(0, 0)
    scatter(0, 0, count, put_own)
    taken_chunks = [0] * CHUNKS
    total = jnp.zeros((1, count), F32)
    for j in range(CHUNKS):
        for d in range(2):
            c = order[d][j]
            give(d, reach, c, back.at[1, d]).wait_recv()
            value = mix[piece(c)] + xbuf[2 * reach - 1 + d, piece(c)].astype(F32)
            taken_chunks[c] += 1
            if taken_chunks[c] == 1:
                mix[piece(c)] = value
            else:
                mixed_ref[piece(c)] = (value * post_ref[...]).astype(BF16)
                total = total + squares_of(c, value)
    squares[1, me] = total
    scale_ref[...] = jnp.broadcast_to(exchange_squares(1), (8, count))
    for d in range(2):
        sent(back.at[0, d], rs.at[d, reach % 2])


def finish_kernel(mixed_ref, scale_ref, out_ref):
    shape = (mixed_ref.shape[0],) * 2
    same = iota(shape, 0) == iota(shape, 1)
    column = jnp.sum(jnp.where(same, scale_ref[0:1], 0.0), axis=1, keepdims=True)
    out_ref[...] = (mixed_ref[...].astype(F32) * column).astype(BF16)


def per_device(
    tokens,
    routes,
    route_weights,
    pre_gain,
    expert_gate,
    expert_up,
    expert_down,
    shared_gate,
    shared_up,
    shared_down,
    post_gain,
):
    members, groups = lax.axis_size("tp"), lax.axis_size("ep")
    count, width = tokens.shape
    fanout = routes.shape[1]
    experts, _, units = expert_gate.shape
    cap = 2 * count * fanout // (experts * groups)
    ring = tuple(ring_of(groups, members // 2))
    reach, wide = groups // 2, members // 2
    slots = experts * cap
    most = max(2 * slots, slots + count)
    share = units // members
    cfg = (groups, members, experts, cap, fanout, ring, float(width * members))

    vmem = pl.BlockSpec(memory_space=pltpu.VMEM)
    anywhere = pl.BlockSpec(memory_space=pl.ANY)
    dma = pltpu.SemaphoreType.DMA
    mixed, scale = pl.pallas_call(
        functools.partial(layer_kernel, cfg),
        out_shape=[
            pltpu.VMEM((count, width), BF16),
            pltpu.VMEM((8, count), F32),
        ],
        in_specs=[anywhere] * 11,
        out_specs=[vmem, vmem],
        scratch_shapes=[
            pltpu.VMEM((fanout, count), routes.dtype),
            pltpu.VMEM((fanout, count), F32),
            pltpu.VMEM((1, width), F32),
            pltpu.VMEM((1, width), F32),
            pltpu.VMEM((count, width), BF16),
            pltpu.VMEM((groups + 1, count, width), BF16),
            pltpu.VMEM((groups, -(-(3 * fanout + 3) // 16) * 16, count), BF16),
            pltpu.VMEM(expert_gate.shape, BF16),
            pltpu.VMEM(expert_up.shape, BF16),
            pltpu.VMEM(expert_down.shape, BF16),
            pltpu.VMEM(shared_gate.shape, BF16),
            pltpu.VMEM(shared_up.shape, BF16),
            pltpu.VMEM(shared_down.shape, BF16),
            pltpu.VMEM((experts, 2 * cap, width), BF16),
            pltpu.VMEM((2, slots, count), BF16),
            pltpu.VMEM((3, count, slots), BF16),
            pltpu.VMEM((wide, 2, most, 2 * share), BF16),
            pltpu.VMEM((2, wide, most, 2 * share), BF16),
            pltpu.VMEM((wide, most, 2 * share), BF16),
            pltpu.VMEM((2, wide - 1, most, 2 * share), BF16),
            pltpu.VMEM((reach + 1, wide, 2, most, share), BF16),
            pltpu.VMEM((3, slots, width), BF16),
            pltpu.VMEM((2, 2, count, width), BF16),
            pltpu.VMEM((count, width), BF16),
            pltpu.VMEM((count, width), F32),
            pltpu.VMEM((groups, TABLE, count), F32),
            pltpu.VMEM((groups, TABLE, count), F32),
            pltpu.VMEM((2, most, 128), F32),
            pltpu.VMEM((2, most, 128), F32),
            pltpu.VMEM((count, count), BF16),
            pltpu.VMEM((count, count), BF16),
            pltpu.VMEM((2, members, 1, count), F32),
            dma((4,)),
            dma((CHUNKS,)),
            dma((6,)),
            dma((2, 2)),
            dma((2, reach, CHUNKS)),
            dma((2,)),
            dma((2, reach)),
            dma((2, 3)),
            dma((experts,)),
            dma((2, experts)),
            dma((experts, wide - 1)),
            dma((2, experts, wide - 1)),
            dma((2, experts, wide - 1)),
            dma((2, experts, wide - 1)),
            dma((2, experts)),
            dma((2, experts)),
            dma((members - 1,)),
            dma((members - 1,)),
            pltpu.SemaphoreType.REGULAR((2,)),
        ],
        compiler_params=pltpu.CompilerParams(
            collective_id=0, has_side_effects=True, vmem_limit_bytes=66977792 - 2 * count * width - 32 * count
        ),
        name="layer",
    )(
        tokens,
        routes.T,
        route_weights.T,
        pre_gain[None, :],
        post_gain[None, :],
        expert_gate,
        expert_up,
        expert_down,
        shared_gate,
        shared_up,
        shared_down,
    )
    mixed = pltpu.with_memory_space_constraint(mixed, pltpu.VMEM)
    scale = pltpu.with_memory_space_constraint(scale, pltpu.VMEM)
    block = count // 2
    return pl.pallas_call(
        finish_kernel,
        grid=(2,),
        in_specs=[
            pl.BlockSpec((block, width), lambda c: (c, 0)),
            pl.BlockSpec((8, block), lambda c: (0, c)),
        ],
        out_specs=pl.BlockSpec((block, width), lambda c: (c, 0)),
        out_shape=jax.ShapeDtypeStruct((count, width), BF16),
        name="finish",
    )(mixed, scale)


def solution(mesh):
    in_specs = (
        P("ep", "tp"),
        P("ep", None),
        P("ep", None),
        P("tp"),
        P("ep", "tp", None),
        P("ep", "tp", None),
        P("ep", None, "tp"),
        P("tp", None),
        P("tp", None),
        P(None, "tp"),
        P("tp"),
    )
    return jax.shard_map(
        per_device, mesh=mesh, in_specs=in_specs, out_specs=P("ep", "tp"), check_vma=False
    )
```
